256 devices in a mesh: rep: 2 (over z_hi), fs: 16 (over z_lo, x), tp: 8 (over y, core).
Axes of the slice: x: 4, y: 4, z: 8 (z_hi: 2, z_lo: 4; z = z_hi * 4 + z_lo), core: 2. Of those that a mesh axis runs over, the one named last changes fastest.
Arguments:
- tokens: bfloat16 [32768, 2048], P(('rep', 'fs', 'tp')), may hold values from -6 to 6
- mix_gain: bfloat16 [2048], replicated, may hold values from 0.099609375 to 1.8984375
- gate_proj: bfloat16 [2048, 512], P('fs', 'tp'), may hold values from -0.125 to 0.125
- value_proj: bfloat16 [2048, 512], P('fs', 'tp'), may hold values from -1 to 1
- layer_gain: bfloat16 [512], replicated, may hold values from 0.099609375 to 1.8984375
- layer_shift: bfloat16 [512], replicated, may hold values from -3 to 3
- mix_kernel: bfloat16 [4, 128, 128], replicated, may hold values from -0.5 to 0.5
- mix_offset: bfloat16 [4, 128], replicated, may hold values from -4 to 4
- out_proj: bfloat16 [2048, 512], P('fs', 'tp'), may hold values from -0.25 to 0.25
- ffn_gain: bfloat16 [2048], replicated, may hold values from 0.099609375 to 1.8984375
- ffn_gate: bfloat16 [2048, 5632], P('fs', 'tp'), may hold values from -0.125 to 0.125
- ffn_up: bfloat16 [2048, 5632], P('fs', 'tp'), may hold values from -0.125 to 0.125
- ffn_down: bfloat16 [2048, 5632], P('fs', 'tp'), may hold values from -0.078125 to 0.078125
Outputs:
- layer_out: bfloat16 [32768, 2048], P(('rep', 'fs', 'tp'))
The draws below stay inside these ranges and needn't reach their ends.
All inputs are finite; a program needn't handle non-finite values.
Results may differ from the reference program's by a relative error of at most 0.015.
Values may be sent and summed in bfloat16 or wider, within the bound.
A program may use at most 64 MiB of HBM per device.

```python
import math
import jax
import jax.numpy as jnp
from jax import lax

D = 2048
FF = 5632
W = 512
GROUP_CH = 128
BLOCK = 128
GROUPS = 4
TOKENS = 32768
N_TP = 8


def draw_value_proj(key, part):
    key_entries = jax.random.fold_in(key, 11)
    key_columns = jax.random.fold_in(key, 12)
    column_pos = jnp.arange(W, dtype=jnp.float32) / max(W - 1, 1)
    jitter = jnp.exp(jax.random.uniform(key_columns, (W,), jnp.float32, 0.0, math.log(4.0)))
    entries = jax.random.normal(key_entries, (D, W), jnp.float32)
    trend = jnp.exp(column_pos * math.log(3.0))
    scaled = entries * D ** (-0.5) * trend[None, :] * jitter[None, :]
    return jnp.clip(scaled, -1.0, 1.0).astype(jnp.bfloat16)


def block_levels(key, dims, pieces, least, high):
    def one(axis_at, shards_of):
        steps = jax.random.uniform(jax.random.fold_in(jax.random.fold_in(key, 6), axis_at), (shards_of,), jnp.float32, least / len(pieces), high / len(pieces))
        return jnp.repeat(jnp.exp(steps), dims[axis_at] // shards_of).reshape((-1,) + (1,) * (len(dims) - axis_at - 1))

    loudness = one(*pieces[0])
    for cut in pieces[1:]:
        loudness = loudness * one(*cut)
    return loudness


def normal_values(rng, dims, width, limit, pieces=(), kind=jnp.bfloat16):
    values = width * jax.random.normal(rng, dims, jnp.float32)
    if pieces:
        values = values * block_levels(rng, dims, pieces, -0.22, 0.18)
    return jnp.clip(values, -limit, limit).astype(kind)


def setup_inputs(seed: int = 0) -> dict:
    streams_of = jax.random.split(jax.random.key(seed), 14)
    tokens = normal_values(streams_of[0], (TOKENS, D), 1.0, 6.0, ((0, 256),))
    mix_gain = jnp.clip(1.0 + 0.18 * jax.random.normal(streams_of[1], (D,), jnp.float32), 0.099609375, 1.8984375).astype(jnp.bfloat16)
    gate_proj = normal_values(streams_of[2], (D, W), D ** -0.5, 0.125, ((0, 16), (1, 8)))
    value_proj = draw_value_proj(jax.random.fold_in(streams_of[13], 71), 0)
    layer_gain = jnp.clip(1.0 + 0.18 * jax.random.normal(streams_of[4], (W,), jnp.float32), 0.099609375, 1.8984375).astype(jnp.bfloat16)
    layer_shift = normal_values(streams_of[5], (W,), 0.5, 3.0)
    mix_kernel = normal_values(streams_of[6], (GROUPS, BLOCK, BLOCK), BLOCK ** -0.5, 0.5)
    mix_offset = normal_values(streams_of[7], (GROUPS, BLOCK), 1.0, 4.0)
    out_proj = normal_values(streams_of[8], (D, W), W ** -0.5, 0.25, ((0, 16), (1, 8)))
    ffn_gain = jnp.clip(1.0 + 0.18 * jax.random.normal(streams_of[9], (D,), jnp.float32), 0.099609375, 1.8984375).astype(jnp.bfloat16)
    ffn_gate = normal_values(streams_of[10], (D, FF), D ** -0.5, 0.125, ((0, 16), (1, 8)))
    ffn_up = normal_values(streams_of[11], (D, FF), D ** -0.5, 0.125, ((0, 16), (1, 8)))
    ffn_down = normal_values(streams_of[12], (D, FF), FF ** -0.5, 0.078125, ((0, 16), (1, 8)))
    return dict(tokens=tokens, mix_gain=mix_gain, gate_proj=gate_proj, value_proj=value_proj, layer_gain=layer_gain, layer_shift=layer_shift, mix_kernel=mix_kernel, mix_offset=mix_offset, out_proj=out_proj, ffn_gain=ffn_gain, ffn_gate=ffn_gate, ffn_up=ffn_up, ffn_down=ffn_down)


epsilon = 1e-06

def rms_norm(rows, gain):
    floats = rows.astype(jnp.float32)
    scale = lax.rsqrt(lax.optimization_barrier(jnp.mean(floats * floats, axis=-1, keepdims=True)) + epsilon)
    return (floats * scale * gain.astype(jnp.float32)).astype(jnp.bfloat16)

def reference(tokens, mix_gain, gate_proj, value_proj, layer_gain, layer_shift, mix_kernel, mix_offset, out_proj, ffn_gain, ffn_gate, ffn_up, ffn_down):
    normed = rms_norm(tokens, mix_gain)
    gate_u = jax.nn.gelu(jnp.dot(normed, gate_proj, preferred_element_type=jnp.float32))
    activated = jax.nn.gelu(jnp.dot(normed, value_proj, preferred_element_type=jnp.float32))
    center = lax.optimization_barrier(jnp.sum(activated, axis=-1, keepdims=True)) / W
    spread = lax.optimization_barrier(jnp.sum(activated * activated, axis=-1, keepdims=True)) / W - center * center
    values = ((activated - center) * lax.rsqrt(spread + epsilon) * layer_gain.astype(jnp.float32) + layer_shift.astype(jnp.float32)).astype(jnp.bfloat16)
    causal = jnp.tril(jnp.ones((BLOCK, BLOCK), dtype=bool))
    masked = jnp.where(causal[None], mix_kernel, jnp.zeros_like(mix_kernel))
    blocks = values.reshape(-1, BLOCK, GROUPS, GROUP_CH).astype(jnp.float32)
    mixing = jnp.einsum('gts,nsgc->ntgc', masked.astype(jnp.float32), blocks)
    mixing = mixing + mix_offset.astype(jnp.float32).T[None, :, :, None]
    gated_rows = (gate_u * mixing.reshape(gate_u.shape)).astype(jnp.bfloat16)
    mixer_out = lax.dot_general(gated_rows, out_proj, (((1,), (1,)), ((), ())), preferred_element_type=jnp.float32)
    middle = (tokens.astype(jnp.float32) + mixer_out).astype(jnp.bfloat16)
    normed2 = rms_norm(middle, ffn_gain)
    gate_pre = jnp.dot(normed2, ffn_gate, preferred_element_type=jnp.float32)
    up_pre = jnp.dot(normed2, ffn_up, preferred_element_type=jnp.float32)
    hidden = (jax.nn.silu(gate_pre) * up_pre).astype(jnp.bfloat16)
    run_len = FF // N_TP
    summed = jnp.zeros((tokens.shape[0], D), jnp.float32)
    for run_id in range(N_TP):
        hidden_run = hidden[:, run_id * run_len:(run_id + 1) * run_len]
        weight_run = ffn_down[:, run_id * run_len:(run_id + 1) * run_len]
        partial_value = lax.dot_general(hidden_run, weight_run, (((1,), (1,)), ((), ())), preferred_element_type=jnp.float32)
        summed = summed + partial_value.astype(jnp.bfloat16).astype(jnp.float32)
    return (middle.astype(jnp.float32) + summed).astype(jnp.bfloat16)
```

```python
import functools

import jax
import jax.numpy as jnp
from jax import lax
from jax.experimental import pallas as pl
from jax.experimental.pallas import tpu as pltpu
from jax.sharding import Mesh
from jax.sharding import PartitionSpec as P

AXES = ("rep", "fs_0", "fs_1", "tp_0", "tp_1")
FS = ("fs_0", "fs_1")
TP = ("tp_0", "tp_1")
EPS = 1e-06
N = 4
COPIES = 192
BF, F32 = jnp.bfloat16, jnp.float32


def dot_nt(left, right):
    return lax.dot_general(left, right, (((1,), (1,)), ((), ())), preferred_element_type=F32)


def gelu(v):
    return v * (0.5 * (1.0 + jnp.tanh(0.7978845608028654 * (v + 0.044715 * (v * v * v)))))


def cat(parts, axis):
    return jnp.concatenate(parts, axis=axis) if len(parts) > 1 else parts[0]


def kernel(
    tokens, gate_proj, value_proj, out_proj, ffn_gate, ffn_up, ffn_down, params, mix_kernel,
    out,
    tok, par, mixk, vw, gw, ow, a_gu, b_gu, a_d, b_d, nbuf, middle, xall, hidden, parts, r1, r2,
    lsem, ssem, rsem,
):
    rep = lax.axis_index("rep")
    zi, xi, yi, ci = (lax.axis_index(a) for a in AXES[1:])

    def wrap(i, s):
        return lax.rem(i + (s + N), N)

    def device(axis, s):
        if axis == "z":
            z = lax.rem(rep * N + zi + (s + 2 * N), 2 * N)
            return {"rep": z // N, "fs_0": lax.rem(z, N)}
        if axis == "c":
            return {"tp_1": 1 - ci}
        name, i = {"x": ("fs_1", xi), "y": ("tp_0", yi)}[axis]
        return {name: wrap(i, s)}

    index = {"x": xi, "y": yi, "z": zi}
    sends = []

    def push(axis, s, mine, theirs):
        k = len(sends)
        to = device(axis, s)
        copy = pltpu.make_async_remote_copy(
            mine, mine, ssem.at[k], rsem.at[k], device_id=to, device_id_type=pl.DeviceIdType.MESH
        )
        copy.start()
        sends.append(copy)
        arrival = pltpu.make_async_remote_copy(
            theirs, theirs, ssem.at[k], rsem.at[k], device_id=to,
            device_id_type=pl.DeviceIdType.MESH,
        )
        return arrival.wait_recv

    locals_ = []

    def load(src, dst):
        copy = pltpu.make_async_copy(src, dst, lsem.at[len(locals_)])
        copy.start()
        locals_.append(copy)
        return copy.wait

    half = a_d.shape[-2]
    own_v = load(value_proj, vw.at[ci, yi, xi, zi])
    own_g = load(gate_proj, gw.at[ci, xi, zi, yi])
    own_o = load(out_proj, ow.at[ci, zi, yi, xi])
    own_gu = [
        load(ffn_gate.at[pl.ds(0, half)], a_gu.at[ci, xi, zi, 0]),
        load(ffn_up.at[pl.ds(0, half)], a_gu.at[ci, xi, zi, 1]),
        load(ffn_gate.at[pl.ds(half, half)], b_gu.at[ci, zi, xi, 0]),
        load(ffn_up.at[pl.ds(half, half)], b_gu.at[ci, zi, xi, 1]),
    ]
    got_tok = load(tokens, tok)
    got_par = load(params, par)
    own_d = [
        load(ffn_down.at[pl.ds(0, half)], a_d.at[ci, xi, zi]),
        load(ffn_down.at[pl.ds(half, half)], b_d.at[ci, zi, xi]),
    ]
    got_mixk = load(mix_kernel, mixk)

    barrier = pltpu.get_barrier_semaphore()
    greeted = [(a, s) for a in "xyz" for s in (1, -1, 2)] + [("z", -2), ("c", 1)]
    for a, s in greeted:
        pl.semaphore_signal(
            barrier, inc=1, device_id=device(a, s), device_id_type=pl.DeviceIdType.MESH
        )
    pl.semaphore_wait(barrier, len(greeted))

    def direct(axis, group, halves):
        i = index[axis]
        got = [
            push(axis, 1, group(i), group(wrap(i, -1))),
            push(axis, -1, group(i), group(wrap(i, 1))),
        ]
        far = wrap(i, 2)
        if axis == "z":
            got += [push(axis, 2, halves(i, 0), halves(far, 0)),
                    push(axis, -2, halves(i, 1), halves(far, 1))]
        else:
            got += [push(axis, 2, group(i), group(far))]
        return got

    class Ring:
        def __init__(self, axis, halves):
            self.axis, self.halves, self.i = axis, halves, index[axis]
            i = self.i
            before, after = wrap(i, -1), wrap(i, 1)
            self.first = [push(axis, 1, halves(i, 0), halves(before, 0)),
                          push(axis, -1, halves(i, 1), halves(after, 1))]
            self.second = [push(axis, 1, halves(i, 1), halves(before, 1)),
                           push(axis, -1, halves(i, 0), halves(after, 0))]

        def relay(self):
            i, h = self.i, self.halves
            before, after, far = wrap(i, -1), wrap(i, 1), wrap(i, 2)
            self.first[0]()
            up = push(self.axis, 1, h(before, 0), h(far, 0))
            self.first[1]()
            down = push(self.axis, -1, h(after, 1), h(far, 1))
            self.last = [up, down]

        def near(self):
            for w in self.second:
                w()

        def end(self):
            for w in self.last:
                w()

    def pair(n):
        return lambda h: pl.ds(h * (n // 2), n // 2)

    rows = pair(vw.shape[-2])
    two = pair(N)
    own_v()
    v1 = direct("z", lambda i: vw.at[ci, yi, xi, i], lambda i, h: vw.at[ci, yi, xi, i, rows(h)])
    own_g()
    g1 = direct("y", lambda i: gw.at[ci, xi, zi, i], None)
    own_o()
    o1 = direct("x", lambda i: ow.at[ci, zi, yi, i], None)
    for w in v1:
        w()
    v2 = direct("x", lambda i: vw.at[ci, yi, i], None)
    for w in g1:
        w()
    g2 = direct("z", lambda i: gw.at[ci, xi, i], lambda i, h: gw.at[ci, xi, i, two(h)])
    for w in o1:
        w()
    o2 = direct("y", lambda i: ow.at[ci, zi, i], None)

    for w in own_gu:
        w()
    agu1 = Ring("z", lambda i, h: a_gu.at[ci, xi, i, h])
    bgu1 = Ring("x", lambda i, h: b_gu.at[ci, zi, i, h])

    fwd_v, fwd_g, fwd_o = [], [], []

    def forward(keep, ref_of):
        keep.append(push("c", 1, ref_of(ci), ref_of(1 - ci)))

    for w in v2:
        w()
    v3 = Ring("y", lambda i, h: vw.at[ci, i, two(h)])
    forward(fwd_v, lambda c: vw.at[c, yi])
    for w in g2:
        w()
    g3 = Ring("x", lambda i, h: gw.at[ci, i, two(h)])
    forward(fwd_g, lambda c: gw.at[c, xi])
    for w in o2:
        w()
    o3 = Ring("z", lambda i, h: ow.at[ci, i, two(h)])
    forward(fwd_o, lambda c: ow.at[c, zi])

    agu1.relay()
    bgu1.relay()
    v3.relay()
    g3.relay()
    o3.relay()
    agu1.near()
    bgu1.near()
    agu1.end()
    bgu1.end()
    agu2 = Ring("x", lambda i, h: a_gu.at[ci, i, two(h)])
    bgu2 = Ring("z", lambda i, h: b_gu.at[ci, i, two(h)])
    fwd_gu = []
    forward(fwd_gu, lambda c: a_gu.at[c, xi])
    forward(fwd_gu, lambda c: b_gu.at[c, zi])
    for w in own_d:
        w()
    ad1 = Ring("z", lambda i, h: a_d.at[ci, xi, i, pl.ds(h * (half // 2), half // 2)])
    bd1 = Ring("x", lambda i, h: b_d.at[ci, zi, i, pl.ds(h * (half // 2), half // 2)])

    def finish(ring, keep, ref, i):
        ring.near()
        forward(keep, lambda c: ref.at[c, wrap(i, -1)])
        forward(keep, lambda c: ref.at[c, wrap(i, 1)])
        ring.end()
        forward(keep, lambda c: ref.at[c, wrap(i, 2)])

    got_tok()
    got_par()
    got_mixk()
    floats = tok[...].astype(F32)
    scale = lax.rsqrt(jnp.mean(floats * floats, axis=-1, keepdims=True) + EPS)
    nbuf[...] = (floats * scale * par[0:1, :]).astype(BF)

    finish(v3, fwd_v, vw, yi)
    finish(g3, fwd_g, gw, xi)
    finish(o3, fwd_o, ow, zi)
    for w in fwd_v:
        w()

    every = [(z, x) for z in range(N) for x in range(N)]

    def project(block, lo):
        cols = [
            cat([block(c, y, z, x) for y in (lo, lo + 1) for c in range(2)], 0) for z, x in every
        ]
        return dot_nt(nbuf[...], cat(cols, 1))

    width = 512
    activated = gelu(cat([project(lambda c, y, z, x: vw[c, y, x, z], lo) for lo in (0, 2)], 1))
    center = jnp.sum(activated, axis=-1, keepdims=True) / width
    spread = jnp.sum(activated * activated, axis=-1, keepdims=True) / width - center * center
    values = (
        (activated - center) * lax.rsqrt(spread + EPS) * par[2:3, 0:width]
        + par[2:3, width : 2 * width]
    ).astype(BF)
    span, groups = mixk.shape[1], mixk.shape[0]
    t_pos = lax.broadcasted_iota(jnp.int32, (span, span), 0)
    s_pos = lax.broadcasted_iota(jnp.int32, (span, span), 1)
    mixing = []
    for g in range(groups):
        masked = jnp.where(s_pos <= t_pos, mixk[g].astype(F32), 0.0).astype(BF)
        offset_row = par[2:3, 2 * width + g * span : 2 * width + (g + 1) * span]
        offset = jnp.sum(jnp.where(s_pos == t_pos, offset_row, 0.0), axis=-1, keepdims=True)
        mixing.append(
            jnp.dot(masked, values[:, g * span : (g + 1) * span], preferred_element_type=F32)
            + offset
        )
    for w in fwd_g:
        w()
    gate_u = gelu(cat([project(lambda c, y, z, x: gw[c, x, z, y], lo) for lo in (0, 2)], 1))
    gated = (gate_u * cat(mixing, 1)).astype(BF)
    for w in fwd_o:
        w()
    total = jnp.zeros((span, 1), F32)
    lane = 128
    for z in range(N):
        weights = cat(
            [
                cat([ow[c, z, y, x] for y in range(N) for c in range(2)], 0)
                for x in range(N)
            ],
            1,
        )
        cols = slice(z * N * lane, (z + 1) * N * lane)
        mid = (
            tok[:, cols].astype(F32) + jnp.dot(gated, weights, preferred_element_type=F32)
        ).astype(BF)
        middle[:, cols] = mid
        mid = mid.astype(F32)
        total += jnp.sum(mid * mid, axis=-1, keepdims=True)
    width2 = middle.shape[1]
    scale2 = lax.rsqrt(total / width2 + EPS)
    xall[yi] = (middle[...].astype(F32) * scale2 * par[1:2, :]).astype(BF)

    toks = Ring("y", lambda i, h: xall.at[i, pl.ds(h * (span // 2), span // 2)])

    ad1.relay()
    bd1.relay()
    agu2.relay()
    bgu2.relay()
    ad1.near()
    bd1.near()
    ad1.end()
    bd1.end()

    order = [zi, wrap(zi, -1), wrap(zi, 1), wrap(zi, 2)]
    before, after, far = wrap(xi, -1), wrap(xi, 1), wrap(xi, 2)
    hr = half // 2
    bd2 = Ring("z", lambda i, h: b_d.at[ci, i, two(h)])
    ad2 = []
    for z in order:
        ad2.append([push("x", 1, a_d.at[ci, xi, z], a_d.at[ci, before, z]),
                    push("x", -1, a_d.at[ci, xi, z], a_d.at[ci, after, z])])
    ad2_last = []

    def down_relay(k):
        z = order[k]
        ad2[k][0]()
        up = push("x", 1, a_d.at[ci, before, z, pl.ds(0, hr)], a_d.at[ci, far, z, pl.ds(0, hr)])
        ad2[k][1]()
        down = push(
            "x", -1, a_d.at[ci, after, z, pl.ds(hr, hr)], a_d.at[ci, far, z, pl.ds(hr, hr)]
        )
        ad2_last.append([up, down])

    toks.relay()
    finish(agu2, fwd_gu, a_gu, xi)
    finish(bgu2, fwd_gu, b_gu, zi)
    toks.near()
    toks.end()
    for w in fwd_gu:
        w()

    full = 4 * half

    def unit_rows(which, lo, hi):
        pieces = []
        for seg in range(4):
            a, b = max(lo, seg * half), min(hi, (seg + 1) * half)
            if a < b:
                c, h = divmod(seg, 2)
                r = slice(a - seg * half, b - seg * half)
                ref = (a_gu, b_gu)[h]
                pieces.append(
                    cat(
                        [
                            ref[(c, x, z) + (which, r)] if h == 0 else ref[(c, z, x) + (which, r)]
                            for z, x in every
                        ],
                        1,
                    )
                )
        return cat(pieces, 0)

    rows_all = xall.reshape(N * span, width2)
    step = 256
    relayed = 0
    for lo in range(0, full, step):
        hi = min(lo + step, full)
        if hi - lo == step:
            gate_pre = dot_nt(rows_all[...], unit_rows(0, lo, hi))
            up_pre = dot_nt(rows_all[...], unit_rows(1, lo, hi))
        else:
            both = dot_nt(
                rows_all[...], cat([unit_rows(0, lo, hi), unit_rows(1, lo, hi)], 0)
            )
            gate_pre, up_pre = both[:, : hi - lo], both[:, hi - lo :]
        hidden[:, lo:hi] = (gate_pre * lax.logistic(gate_pre) * up_pre).astype(BF)
        if lo == 2 * step:
            bd2.relay()
        if lo == 4 * step:
            down_relay(0)

    got_r1, got_r2, ahead, back = {}, {}, wrap(yi, 1), wrap(yi, -1)
    opposite = wrap(yi, 2)

    def sum_first(k):
        z = order[k]
        got_r1[k] = [
            send_to("y", 1, parts.at[opposite, z, two(0)], r1.at[0, k]),
            send_to("y", -1, parts.at[opposite, z, two(1)], r1.at[1, k]),
        ]
        got_r2[k] = [
            send_to("y", 1, parts.at[ahead, z, two(1)], r2.at[0, k, two(1)]),
            send_to("y", -1, parts.at[back, z, two(0)], r2.at[1, k, two(0)]),
        ]

    def send_to(axis, s, src, dst):
        k = len(sends)
        copy = pltpu.make_async_remote_copy(
            src, dst, ssem.at[k], rsem.at[k], device_id=device(axis, s),
            device_id_type=pl.DeviceIdType.MESH,
        )
        copy.start()
        sends.append(copy)
        return copy.wait_recv

    def sum_second(k):
        z = order[k]
        got_r1[k][0]()
        parts[ahead, z, two(0)] = (
            parts[ahead, z, two(0)].astype(F32) + r1[0, k].astype(F32)
        ).astype(BF)
        got_r2[k].append(send_to("y", 1, parts.at[ahead, z, two(0)], r2.at[0, k, two(0)]))
        got_r1[k][1]()
        parts[back, z, two(1)] = (
            parts[back, z, two(1)].astype(F32) + r1[1, k].astype(F32)
        ).astype(BF)
        got_r2[k].append(send_to("y", -1, parts.at[back, z, two(1)], r2.at[1, k, two(1)]))

    def sum_last(k):
        z = order[k]
        for w in got_r2[k]:
            w()
        for x in range(N):
            summed = (
                parts[yi, z, x].astype(F32) + r2[0, k, x].astype(F32) + r2[1, k, x].astype(F32)
            )
            cols = pl.ds(pl.multiple_of((z * N + x) * lane, lane), lane)
            out[:, cols] = (middle[:, cols].astype(F32) + summed).astype(BF)

    def chunk(k):
        z = order[k]
        if k == 1:
            bd2.near()
        if k == 3:
            bd2.end()
        for w in ad2_last[k]:
            w()
        fwd = []
        forward(fwd, lambda c: a_d.at[c, :, z])
        forward(fwd, lambda c: b_d.at[c, z])
        if k + 1 < N:
            down_relay(k + 1)
        for w in fwd:
            w()
        for x2 in range(0, N, 2):
            weights = cat(
                [
                    cat([ref for c in range(2) for ref in (a_d[c, x, z], b_d[c, z, x])], 0)
                    for x in (x2, x2 + 1)
                ],
                1,
            )
            result = jnp.dot(hidden[...], weights, preferred_element_type=F32).astype(BF)
            for y in range(N):
                for j in range(2):
                    parts[y, z, x2 + j] = result[
                        y * span : (y + 1) * span, j * lane : (j + 1) * lane
                    ]

    for k in range(N):
        chunk(k)
        sum_first(k)
        if k:
            sum_second(k - 1)
        if k > 1:
            sum_last(k - 2)
    sum_second(N - 1)
    sum_last(N - 2)
    sum_last(N - 1)
    for copy in sends:
        copy.wait_send()


def per_device(
    tokens, mix_gain, gate_proj, value_proj, layer_gain, layer_shift, mix_kernel, mix_offset,
    out_proj, ffn_gain, ffn_gate, ffn_up, ffn_down,
):
    span, width = tokens.shape
    units, lane = ffn_gate.shape[1], ffn_gate.shape[0]
    channels = layer_gain.shape[0]
    local = gate_proj.shape[1]
    half = units // 2
    small = jnp.concatenate(
        [layer_gain, layer_shift, mix_offset.reshape(-1)]
        + [jnp.zeros((width - 3 * channels,), BF)]
    )
    params = jnp.stack([mix_gain, ffn_gain, small] + [jnp.zeros_like(mix_gain)] * 5).astype(F32)
    anywhere = pl.BlockSpec(memory_space=pl.ANY)
    return pl.pallas_call(
        kernel,
        out_shape=jax.ShapeDtypeStruct(tokens.shape, BF),
        in_specs=[anywhere] * 9,
        out_specs=pl.BlockSpec(memory_space=pltpu.VMEM),
        scratch_shapes=[
            pltpu.VMEM((span, width), BF),
            pltpu.VMEM(params.shape, F32),
            pltpu.VMEM(mix_kernel.shape, BF),
            pltpu.VMEM((2, N, N, N, local, lane), BF),
            pltpu.VMEM((2, N, N, N, local, lane), BF),
            pltpu.VMEM((2, N, N, N, local, lane), BF),
            pltpu.VMEM((2, N, N, 2, half, lane), BF),
            pltpu.VMEM((2, N, N, 2, half, lane), BF),
            pltpu.VMEM((2, N, N, half, lane), BF),
            pltpu.VMEM((2, N, N, half, lane), BF),
            pltpu.VMEM((span, width), BF),
            pltpu.VMEM((span, width), BF),
            pltpu.VMEM((N, span, width), BF),
            pltpu.VMEM((N * span, 2 * units), BF),
            pltpu.VMEM((N, N, N, span, lane), BF),
            pltpu.VMEM((2, N, N // 2, span, lane), BF),
            pltpu.VMEM((2, N, N, span, lane), BF),
            pltpu.SemaphoreType.DMA((16,)),
            pltpu.SemaphoreType.DMA((COPIES,)),
            pltpu.SemaphoreType.DMA((COPIES,)),
        ],
        compiler_params=pltpu.CompilerParams(
            collective_id=0, has_side_effects=True, vmem_limit_bytes=63 * 2**20
        ),
    )(
        tokens, gate_proj.T, value_proj.T, out_proj.T, ffn_gate.T, ffn_up.T, ffn_down.T, params,
        mix_kernel,
    )


def solution(mesh):
    torus = Mesh(mesh.devices.reshape(mesh.shape["rep"], 4, 4, 4, 2), AXES)
    return jax.shard_map(
        per_device,
        mesh=torus,
        in_specs=(
            P(AXES, None), P(), P(FS, TP), P(FS, TP), P(), P(), P(), P(), P(FS, TP), P(),
            P(FS, TP), P(FS, TP), P(FS, TP),
        ),
        out_specs=P(AXES, None),
        check_vma=False,
    )
```

```python
import functools

import jax
import jax.numpy as jnp
from jax import lax
from jax.experimental import pallas as pl
from jax.experimental.pallas import tpu as pltpu
from jax.sharding import Mesh
from jax.sharding import PartitionSpec as P

AXES = ("rep", "fs_0", "fs_1", "tp_0", "tp_1")
FS = ("fs_0", "fs_1")
TP = ("tp_0", "tp_1")
EPS = 1e-06
N = 4
COPIES = 216


def row_waves(half):
    return [(0, 128), (128, 128), (256, half - 256)]

BF, F32 = jnp.bfloat16, jnp.float32


def dot_nt(left, right):
    return lax.dot_general(left, right, (((1,), (1,)), ((), ())), preferred_element_type=F32)


def gelu(v):
    return v * (0.5 * (1.0 + jnp.tanh(0.7978845608028654 * (v + 0.044715 * (v * v * v)))))


def row(ref):
    return ref[...].astype(F32).reshape(1, -1)


def cat(parts, axis):
    return jnp.concatenate(parts, axis=axis) if len(parts) > 1 else parts[0]


def kernel(
    tokens, gate_proj, value_proj, out_proj, ffn_gate, ffn_up, ffn_down, mix_gain, layer_gain,
    layer_shift, mix_kernel, mix_offset, ffn_gain,
    out,
    tok, gain1, gain2, lgain, lshift, mixo, mixk, vw, gw, ow, a_gu, b_gu, a_d, b_d, nbuf, middle, xall, hidden, parts, r1, r2,
    lsem, ssem, rsem,
):
    rep = lax.axis_index("rep")
    zi, xi, yi, ci = (lax.axis_index(a) for a in AXES[1:])

    def wrap(i, s):
        return lax.rem(i + (s + N), N)

    def device(axis, s):
        if axis == "z":
            z = lax.rem(rep * N + zi + (s + 2 * N), 2 * N)
            return {"rep": z // N, "fs_0": lax.rem(z, N)}
        if axis == "c":
            return {"tp_1": 1 - ci}
        name, i = {"x": ("fs_1", xi), "y": ("tp_0", yi)}[axis]
        return {name: wrap(i, s)}

    index = {"x": xi, "y": yi, "z": zi}
    sends = []

    def push(axis, s, mine, theirs):
        k = len(sends)
        to = device(axis, s)
        copy = pltpu.make_async_remote_copy(
            mine, mine, ssem.at[k], rsem.at[k], device_id=to, device_id_type=pl.DeviceIdType.MESH
        )
        copy.start()
        sends.append(copy)
        arrival = pltpu.make_async_remote_copy(
            theirs, theirs, ssem.at[k], rsem.at[k], device_id=to,
            device_id_type=pl.DeviceIdType.MESH,
        )
        return arrival.wait_recv

    locals_ = []

    def load(src, dst):
        copy = pltpu.make_async_copy(src, dst, lsem.at[len(locals_)])
        copy.start()
        locals_.append(copy)
        return copy.wait

    half = a_d.shape[-2]
    hr = half // 2
    waves = row_waves(half)
    half = a_d.shape[-2]
    hr = half // 2
    own_v = load(value_proj, vw.at[ci, yi, xi, zi])
    own_g = load(gate_proj, gw.at[ci, xi, zi, yi])
    own_o = load(out_proj, ow.at[ci, zi, yi, xi])
    own_gu = [
        load(src.at[pl.ds(h * half, half)], dst.at[j])
        for h, dst in ((0, a_gu.at[ci, xi, zi]), (1, b_gu.at[ci, zi, xi]))
        for j, src in ((0, ffn_gate), (1, ffn_up))
    ]
    got_tok = load(tokens, tok)
    own_d = [
        load(ffn_down.at[pl.ds(0, half)], a_d.at[ci, xi, zi]),
        load(ffn_down.at[pl.ds(half, half)], b_d.at[ci, zi, xi]),
    ]
    got_small = [
        load(src, dst)
        for src, dst in (
            (mix_gain, gain1), (layer_gain, lgain), (layer_shift, lshift), (mix_kernel, mixk),
            (mix_offset, mixo), (ffn_gain, gain2),
        )
    ]

    barrier = pltpu.get_barrier_semaphore()
    greeted = [(a, s) for a in "xyz" for s in (1, -1, 2)] + [("z", -2), ("c", 1)]
    for a, s in greeted:
        pl.semaphore_signal(
            barrier, inc=1, device_id=device(a, s), device_id_type=pl.DeviceIdType.MESH
        )
    pl.semaphore_wait(barrier, len(greeted))

    def direct(axis, group, halves):
        i = index[axis]
        got = [
            push(axis, 1, group(i), group(wrap(i, -1))),
            push(axis, -1, group(i), group(wrap(i, 1))),
        ]
        far = wrap(i, 2)
        if axis == "z":
            got += [push(axis, 2, halves(i, 0), halves(far, 0)),
                    push(axis, -2, halves(i, 1), halves(far, 1))]
        else:
            got += [push(axis, 2, group(i), group(far))]
        return got

    class Ring:
        def __init__(self, axis, halves):
            self.axis, self.halves, self.i = axis, halves, index[axis]
            i = self.i
            before, after = wrap(i, -1), wrap(i, 1)
            self.first = [push(axis, 1, halves(i, 0), halves(before, 0)),
                          push(axis, -1, halves(i, 1), halves(after, 1))]
            self.second = [push(axis, 1, halves(i, 1), halves(before, 1)),
                           push(axis, -1, halves(i, 0), halves(after, 0))]

        def relay(self):
            i, h = self.i, self.halves
            before, after, far = wrap(i, -1), wrap(i, 1), wrap(i, 2)
            self.first[0]()
            up = push(self.axis, 1, h(before, 0), h(far, 0))
            self.first[1]()
            down = push(self.axis, -1, h(after, 1), h(far, 1))
            self.last = [up, down]

        def near(self):
            for w in self.second:
                w()

        def end(self):
            for w in self.last:
                w()

    def pair(n):
        return lambda h: pl.ds(h * (n // 2), n // 2)

    rows = pair(vw.shape[-2])
    two = pair(N)
    own_v()
    v1 = direct("z", lambda i: vw.at[ci, yi, xi, i], lambda i, h: vw.at[ci, yi, xi, i, rows(h)])
    own_g()
    g1 = direct("y", lambda i: gw.at[ci, xi, zi, i], None)
    own_o()
    o1 = direct("x", lambda i: ow.at[ci, zi, yi, i], None)

    def wave(ref, w):
        off, count = waves[w]
        return lambda c, i: ref.at[c, i, :, :, pl.ds(off, count)]

    def wave_rings(w):
        off, count = waves[w]
        for ref, i in ((a_gu, xi), (b_gu, zi)):
            forward(fwd_gu[w], lambda c: wave(ref, w)(c, i))
        return (
            Ring("x", lambda i, h: a_gu.at[ci, i, two(h), :, pl.ds(off, count)]),
            Ring("z", lambda i, h: b_gu.at[ci, i, two(h), :, pl.ds(off, count)]),
        )

    def done(waits):
        for w in waits:
            w()

    def forward(keep, ref_of):
        keep.append(push("c", 1, ref_of(ci), ref_of(1 - ci)))

    def group(ref):
        return lambda c, i: ref.at[c, i]

    def finish_near(ring, keep, of, i):
        ring.near()
        forward(keep, lambda c: of(c, wrap(i, -1)))
        forward(keep, lambda c: of(c, wrap(i, 1)))

    def finish_far(ring, keep, of, i):
        ring.end()
        forward(keep, lambda c: of(c, wrap(i, 2)))

    fwd_v, fwd_g, fwd_o, fwd_gu = [], [], [], [[], [], []]
    done(own_gu)
    first = (Ring("z", lambda i, h: a_gu.at[ci, xi, i, h]),
             Ring("x", lambda i, h: b_gu.at[ci, zi, i, h]))
    done(v1)
    v2 = direct("x", lambda i: vw.at[ci, yi, i], None)
    done(g1)
    g2 = direct("z", lambda i: gw.at[ci, xi, i], lambda i, h: gw.at[ci, xi, i, two(h)])
    done(o1)
    o2 = direct("y", lambda i: ow.at[ci, zi, i], None)
    for ring in first:
        ring.relay()
    done(v2)
    v3 = Ring("y", lambda i, h: vw.at[ci, i, two(h)])
    forward(fwd_v, lambda c: vw.at[c, yi])
    done(g2)
    g3 = Ring("x", lambda i, h: gw.at[ci, i, two(h)])
    forward(fwd_g, lambda c: gw.at[c, xi])
    done(o2)
    o3 = Ring("z", lambda i, h: ow.at[ci, i, two(h)])
    forward(fwd_o, lambda c: ow.at[c, zi])

    got_tok()
    done(got_small)
    floats = tok[...].astype(F32)
    scale = lax.rsqrt(jnp.mean(floats * floats, axis=-1, keepdims=True) + EPS)
    nbuf[...] = (floats * scale * row(gain1)).astype(BF)

    v3.relay()
    g3.relay()
    o3.relay()
    for ring in first:
        ring.near()
        ring.end()
    second = [wave_rings(w) for w in range(len(waves))]
    done(own_d)
    ad1 = Ring("z", lambda i, h: a_d.at[ci, xi, i, pl.ds(h * hr, hr)])
    bd1 = Ring("x", lambda i, h: b_d.at[ci, zi, i, pl.ds(h * hr, hr)])
    finish_near(v3, fwd_v, group(vw), yi)
    finish_far(v3, fwd_v, group(vw), yi)
    finish_near(g3, fwd_g, group(gw), xi)
    finish_near(o3, fwd_o, group(ow), zi)
    finish_far(g3, fwd_g, group(gw), xi)
    done(fwd_v)

    every = [(z, x) for z in range(N) for x in range(N)]

    def project(block, lo):
        cols = [
            cat([block(c, y, z, x) for y in (lo, lo + 1) for c in range(2)], 0) for z, x in every
        ]
        return dot_nt(nbuf[...], cat(cols, 1))

    width = 512
    activated = gelu(cat([project(lambda c, y, z, x: vw[c, y, x, z], lo) for lo in (0, 2)], 1))
    center = jnp.sum(activated, axis=-1, keepdims=True) / width
    spread = jnp.sum(activated * activated, axis=-1, keepdims=True) / width - center * center
    values = (
        (activated - center) * lax.rsqrt(spread + EPS) * row(lgain) + row(lshift)
    ).astype(BF)
    finish_far(o3, fwd_o, group(ow), zi)
    span, groups = mixk.shape[1], mixk.shape[0]
    t_pos = lax.broadcasted_iota(jnp.int32, (span, span), 0)
    s_pos = lax.broadcasted_iota(jnp.int32, (span, span), 1)
    mixing = []
    for g in range(groups):
        masked = jnp.where(s_pos <= t_pos, mixk[g].astype(F32), 0.0).astype(BF)
        offset_row = mixo[g : g + 1, :].astype(F32)
        offset = jnp.sum(jnp.where(s_pos == t_pos, offset_row, 0.0), axis=-1, keepdims=True)
        mixing.append(
            jnp.dot(masked, values[:, g * span : (g + 1) * span], preferred_element_type=F32)
            + offset
        )
    done(fwd_g)
    gate_u = gelu(cat([project(lambda c, y, z, x: gw[c, x, z, y], lo) for lo in (0, 2)], 1))
    gated = (gate_u * cat(mixing, 1)).astype(BF)
    done(fwd_o)
    total = jnp.zeros((span, 1), F32)
    lane = 128
    for z in range(N):
        weights = cat(
            [
                cat([ow[c, z, y, x] for y in range(N) for c in range(2)], 0)
                for x in range(N)
            ],
            1,
        )
        cols = slice(z * N * lane, (z + 1) * N * lane)
        mid = (
            tok[:, cols].astype(F32) + jnp.dot(gated, weights, preferred_element_type=F32)
        ).astype(BF)
        middle[:, cols] = mid
        mid = mid.astype(F32)
        total += jnp.sum(mid * mid, axis=-1, keepdims=True)
    width2 = middle.shape[1]
    scale2 = lax.rsqrt(total / width2 + EPS)
    xall[yi] = (middle[...].astype(F32) * scale2 * row(gain2)).astype(BF)

    toks = Ring("y", lambda i, h: xall.at[i, pl.ds(h * (span // 2), span // 2)])

    order = [zi, wrap(zi, -1), wrap(zi, 1), wrap(zi, 2)]
    before, after, far = wrap(xi, -1), wrap(xi, 1), wrap(xi, 2)
    ad2, ad2_last = [], []

    def down_send(k):
        z = order[k]
        ad2.append([push("x", 1, a_d.at[ci, xi, z], a_d.at[ci, before, z]),
                    push("x", -1, a_d.at[ci, xi, z], a_d.at[ci, after, z])])

    def down_relay(k):
        z = order[k]
        ad2[k][0]()
        up = push("x", 1, a_d.at[ci, before, z, pl.ds(0, hr)], a_d.at[ci, far, z, pl.ds(0, hr)])
        ad2[k][1]()
        down = push(
            "x", -1, a_d.at[ci, after, z, pl.ds(hr, hr)], a_d.at[ci, far, z, pl.ds(hr, hr)]
        )
        ad2_last.append([up, down])

    def finish_wave(w):
        for finish in (finish_near, finish_far):
            finish(second[w][0], fwd_gu[w], wave(a_gu, w), xi)
            finish(second[w][1], fwd_gu[w], wave(b_gu, w), zi)

    for ring in second[0]:
        ring.relay()
    for ring in second[1]:
        ring.relay()
    toks.relay()
    for ring in second[2]:
        ring.relay()
    for ring in (ad1, bd1):
        ring.relay()
    down_send(0)
    for ring in (ad1, bd1):
        ring.near()
    down_send(1)
    down_send(2)
    finish_wave(0)
    finish_wave(1)
    toks.near()
    toks.end()
    done(fwd_gu[0])

    def unit_rows(w, which, lo, hi):
        count = waves[w][1]
        pieces = []
        for seg in range(4):
            a, b = max(lo, seg * count), min(hi, (seg + 1) * count)
            if a < b:
                c, h = divmod(seg, 2)
                r = slice(waves[w][0] + a - seg * count, waves[w][0] + b - seg * count)
                ref = (a_gu, b_gu)[h]
                pieces.append(
                    cat(
                        [
                            ref[(c, x, z) + (which, r)] if h == 0 else ref[(c, z, x) + (which, r)]
                            for z, x in every
                        ],
                        1,
                    )
                )
        return cat(pieces, 0)

    rows_all = xall.reshape(N * span, width2)
    step = 256

    def hidden_tile(w, lo):
        count = 4 * waves[w][1]
        hi = min(lo + step, count)
        if hi - lo == step:
            gate_pre = dot_nt(rows_all[...], unit_rows(w, 0, lo, hi))
            up_pre = dot_nt(rows_all[...], unit_rows(w, 1, lo, hi))
        else:
            both = dot_nt(
                rows_all[...], cat([unit_rows(w, 0, lo, hi), unit_rows(w, 1, lo, hi)], 0)
            )
            gate_pre, up_pre = both[:, : hi - lo], both[:, hi - lo :]
        at = 4 * waves[w][0]
        hidden[:, at + lo : at + hi] = (gate_pre * lax.logistic(gate_pre) * up_pre).astype(BF)

    for lo in range(0, 4 * waves[0][1], step):
        hidden_tile(0, lo)
    for ring in (ad1, bd1):
        ring.end()
    bd2 = Ring("z", lambda i, h: b_d.at[ci, i, two(h)])
    down_send(3)
    finish_wave(2)
    done(fwd_gu[1])
    hidden_tile(1, 0)
    down_relay(0)
    hidden_tile(1, step)
    done(fwd_gu[2])
    hidden_tile(2, 0)
    fwd_d = []

    def down_forward(k):
        z = order[k]
        if k == 1:
            bd2.relay()
            bd2.near()
        if k == 3:
            bd2.end()
        for w in ad2_last[k]:
            w()
        fwd = []
        forward(fwd, lambda c: a_d.at[c, :, z])
        forward(fwd, lambda c: b_d.at[c, z])
        fwd_d.append(fwd)

    down_forward(0)
    hidden_tile(2, step)
    down_relay(1)

    got_r1, got_r2, ahead, back = {}, {}, wrap(yi, 1), wrap(yi, -1)
    opposite = wrap(yi, 2)

    def sum_first(r):
        z, lo, mid, hi = rounds[r]
        low, high = pl.ds(lo, mid - lo), pl.ds(mid, hi - mid)
        got_r1[r] = [
            send_to("y", 1, parts.at[opposite, z, low], r1.at[0, z, low]),
            send_to("y", -1, parts.at[opposite, z, high], r1.at[1, z, high]),
        ]
        got_r2[r] = [
            send_to("y", 1, parts.at[ahead, z, high], r2.at[0, z, high]),
            send_to("y", -1, parts.at[back, z, low], r2.at[1, z, low]),
        ]

    def send_to(axis, s, src, dst):
        k = len(sends)
        copy = pltpu.make_async_remote_copy(
            src, dst, ssem.at[k], rsem.at[k], device_id=device(axis, s),
            device_id_type=pl.DeviceIdType.MESH,
        )
        copy.start()
        sends.append(copy)
        return copy.wait_recv

    def sum_second(r):
        z, lo, mid, hi = rounds[r]
        low, high = pl.ds(lo, mid - lo), pl.ds(mid, hi - mid)
        got_r1[r][0]()
        parts[ahead, z, low] = (
            parts[ahead, z, low].astype(F32) + r1[0, z, low].astype(F32)
        ).astype(BF)
        got_r2[r].append(send_to("y", 1, parts.at[ahead, z, low], r2.at[0, z, low]))
        got_r1[r][1]()
        parts[back, z, high] = (
            parts[back, z, high].astype(F32) + r1[1, z, high].astype(F32)
        ).astype(BF)
        got_r2[r].append(send_to("y", -1, parts.at[back, z, high], r2.at[1, z, high]))

    def sum_last(r):
        z, lo, mid, hi = rounds[r]
        done(got_r2[r])
        for x in range(lo, hi):
            summed = (
                parts[yi, z, x].astype(F32) + r2[0, z, x].astype(F32) + r2[1, z, x].astype(F32)
            )
            cols = pl.ds(pl.multiple_of((z * N + x) * lane, lane), lane)
            out[:, cols] = (middle[:, cols].astype(F32) + summed).astype(BF)

    def multiply(z, x2):
        weights = cat(
            [
                cat(
                    [
                        ref
                        for off, count in waves
                        for c in range(2)
                        for ref in (a_d[c, x, z, off : off + count], b_d[c, z, x, off : off + count])
                    ],
                    0,
                )
                for x in (x2, x2 + 1)
            ],
            1,
        )
        result = jnp.dot(hidden[...], weights, preferred_element_type=F32).astype(BF)
        for y in range(N):
            for j in range(2):
                parts[y, z, x2 + j] = result[y * span : (y + 1) * span, j * lane : (j + 1) * lane]

    rounds = [(order[0], 0, 2, 4), (order[1], 0, 2, 4), (order[2], 0, 2, 4),
              (order[3], 0, 1, 2), (order[3], 2, 3, 4)]
    for k in range(N - 1):
        done(fwd_d[k])
        multiply(order[k], 0)
        multiply(order[k], 2)
        sum_first(k)
        down_forward(k + 1)
        if k + 2 < N:
            down_relay(k + 2)
        if k:
            sum_second(k - 1)
    done(fwd_d[3])
    multiply(order[3], 0)
    sum_first(3)
    multiply(order[3], 2)
    sum_first(4)
    sum_second(2)
    sum_last(0)
    sum_second(3)
    sum_second(4)
    sum_last(1)
    sum_last(2)
    sum_last(3)
    sum_last(4)
    assert len(sends) <= COPIES
    for copy in sends:
        copy.wait_send()


def per_device(
    tokens, mix_gain, gate_proj, value_proj, layer_gain, layer_shift, mix_kernel, mix_offset,
    out_proj, ffn_gain, ffn_gate, ffn_up, ffn_down,
):
    span, width = tokens.shape
    units, lane = ffn_gate.shape[1], ffn_gate.shape[0]
    local = gate_proj.shape[1]
    half = units // 2
    anywhere = pl.BlockSpec(memory_space=pl.ANY)
    return pl.pallas_call(
        kernel,
        out_shape=jax.ShapeDtypeStruct(tokens.shape, BF),
        in_specs=[anywhere] * 13,
        out_specs=pl.BlockSpec(memory_space=pltpu.VMEM),
        scratch_shapes=[
            pltpu.VMEM((span, width), BF),
            pltpu.VMEM(mix_gain.shape, BF),
            pltpu.VMEM(ffn_gain.shape, BF),
            pltpu.VMEM(layer_gain.shape, BF),
            pltpu.VMEM(layer_shift.shape, BF),
            pltpu.VMEM(mix_offset.shape, BF),
            pltpu.VMEM(mix_kernel.shape, BF),
            pltpu.VMEM((2, N, N, N, local, lane), BF),
            pltpu.VMEM((2, N, N, N, local, lane), BF),
            pltpu.VMEM((2, N, N, N, local, lane), BF),
            pltpu.VMEM((2, N, N, 2, half, lane), BF),
            pltpu.VMEM((2, N, N, 2, half, lane), BF),
            pltpu.VMEM((2, N, N, half, lane), BF),
            pltpu.VMEM((2, N, N, half, lane), BF),
            pltpu.VMEM((span, width), BF),
            pltpu.VMEM((span, width), BF),
            pltpu.VMEM((N, span, width), BF),
            pltpu.VMEM((N * span, 2 * units), BF),
            pltpu.VMEM((N, N, N, span, lane), BF),
            pltpu.VMEM((2, N, N, span, lane), BF),
            pltpu.VMEM((2, N, N, span, lane), BF),
            pltpu.SemaphoreType.DMA((24,)),
            pltpu.SemaphoreType.DMA((COPIES,)),
            pltpu.SemaphoreType.DMA((COPIES,)),
        ],
        compiler_params=pltpu.CompilerParams(
            collective_id=0, has_side_effects=True, vmem_limit_bytes=63 * 2**20
        ),
    )(
        tokens, gate_proj.T, value_proj.T, out_proj.T, ffn_gate.T, ffn_up.T, ffn_down.T,
        mix_gain, layer_gain, layer_shift, mix_kernel, mix_offset, ffn_gain,
    )


def solution(mesh):
    torus = Mesh(mesh.devices.reshape(mesh.shape["rep"], 4, 4, 4, 2), AXES)
    return jax.shard_map(
        per_device,
        mesh=torus,
        in_specs=(
            P(AXES, None), P(), P(FS, TP), P(FS, TP), P(), P(), P(), P(), P(FS, TP), P(),
            P(FS, TP), P(FS, TP), P(FS, TP),
        ),
        out_specs=P(AXES, None),
        check_vma=False,
    )
```

```python
import functools

import jax
import jax.numpy as jnp
from jax import lax
from jax.experimental import pallas as pl
from jax.experimental.pallas import tpu as pltpu
from jax.sharding import Mesh
from jax.sharding import PartitionSpec as P

AXES = ("rep", "fs_0", "fs_1", "tp_0", "tp_1")
FS = ("fs_0", "fs_1")
TP = ("tp_0", "tp_1")
EPS = 1e-06
N = 4
COPIES = 216


def row_waves(half):
    return [(0, 128), (128, 128), (256, half - 256)]

BF, F32 = jnp.bfloat16, jnp.float32


def dot_nt(left, right):
    return lax.dot_general(left, right, (((1,), (1,)), ((), ())), preferred_element_type=F32)


def gelu(v):
    return v * (0.5 * (1.0 + jnp.tanh(0.7978845608028654 * (v + 0.044715 * (v * v * v)))))


def row(ref):
    return ref[...].astype(F32).reshape(1, -1)


def cat(parts, axis):
    return jnp.concatenate(parts, axis=axis) if len(parts) > 1 else parts[0]


def kernel(
    tokens, gate_proj, value_proj, out_proj, ffn_gate, ffn_up, ffn_down, mix_gain, layer_gain,
    layer_shift, mix_kernel, mix_offset, ffn_gain,
    out,
    tok, gain1, gain2, lgain, lshift, mixo, mixk, vw, gw, ow, a_gu, b_gu, a_d, b_d, nbuf, middle, xall, hidden, parts, r1, r2,
    lsem, ssem, rsem,
):
    rep = lax.axis_index("rep")
    zi, xi, yi, ci = (lax.axis_index(a) for a in AXES[1:])

    def wrap(i, s):
        return lax.rem(i + (s + N), N)

    def device(axis, s):
        if axis == "z":
            z = lax.rem(rep * N + zi + (s + 2 * N), 2 * N)
            return {"rep": z // N, "fs_0": lax.rem(z, N)}
        if axis == "c":
            return {"tp_1": 1 - ci}
        name, i = {"x": ("fs_1", xi), "y": ("tp_0", yi)}[axis]
        return {name: wrap(i, s)}

    index = {"x": xi, "y": yi, "z": zi}
    sends = []

    def push(axis, s, mine, theirs):
        k = len(sends)
        to = device(axis, s)
        copy = pltpu.make_async_remote_copy(
            mine, mine, ssem.at[k], rsem.at[k], device_id=to, device_id_type=pl.DeviceIdType.MESH
        )
        copy.start()
        sends.append(copy)
        arrival = pltpu.make_async_remote_copy(
            theirs, theirs, ssem.at[k], rsem.at[k], device_id=to,
            device_id_type=pl.DeviceIdType.MESH,
        )
        return arrival.wait_recv

    locals_ = []

    def load(src, dst):
        copy = pltpu.make_async_copy(src, dst, lsem.at[len(locals_)])
        copy.start()
        locals_.append(copy)
        return copy.wait

    half = a_d.shape[-2]
    hr = half // 2
    waves = row_waves(half)
    own_v = load(value_proj, vw.at[ci, yi, xi, zi])
    own_g = load(gate_proj, gw.at[ci, xi, zi, yi])
    own_o = load(out_proj, ow.at[ci, zi, yi, xi])
    own_gu = [
        load(src.at[pl.ds(h * half, half)], dst.at[j])
        for h, dst in ((0, a_gu.at[ci, xi, zi]), (1, b_gu.at[ci, zi, xi]))
        for j, src in ((0, ffn_gate), (1, ffn_up))
    ]
    got_tok = load(tokens, tok)
    own_d = [
        load(ffn_down.at[pl.ds(0, half)], a_d.at[ci, xi, zi]),
        load(ffn_down.at[pl.ds(half, half)], b_d.at[ci, zi, xi]),
    ]
    got_small = [
        load(src, dst)
        for src, dst in (
            (mix_gain, gain1), (layer_gain, lgain), (layer_shift, lshift), (mix_kernel, mixk),
            (mix_offset, mixo), (ffn_gain, gain2),
        )
    ]

    barrier = pltpu.get_barrier_semaphore()
    greeted = [(a, s) for a in "xyz" for s in (1, -1, 2)] + [("z", -2), ("c", 1)]
    for a, s in greeted:
        pl.semaphore_signal(
            barrier, inc=1, device_id=device(a, s), device_id_type=pl.DeviceIdType.MESH
        )
    pl.semaphore_wait(barrier, len(greeted))

    def direct(axis, group, halves):
        i = index[axis]
        got = [
            push(axis, 1, group(i), group(wrap(i, -1))),
            push(axis, -1, group(i), group(wrap(i, 1))),
        ]
        far = wrap(i, 2)
        if axis == "z":
            got += [push(axis, 2, halves(i, 0), halves(far, 0)),
                    push(axis, -2, halves(i, 1), halves(far, 1))]
        else:
            got += [push(axis, 2, group(i), group(far))]
        return got

    class Ring:
        def __init__(self, axis, halves):
            self.axis, self.halves, self.i = axis, halves, index[axis]
            i = self.i
            before, after = wrap(i, -1), wrap(i, 1)
            self.first = [push(axis, 1, halves(i, 0), halves(before, 0)),
                          push(axis, -1, halves(i, 1), halves(after, 1))]
            self.second = [push(axis, 1, halves(i, 1), halves(before, 1)),
                           push(axis, -1, halves(i, 0), halves(after, 0))]

        def relay(self):
            i, h = self.i, self.halves
            before, after, far = wrap(i, -1), wrap(i, 1), wrap(i, 2)
            self.first[0]()
            up = push(self.axis, 1, h(before, 0), h(far, 0))
            self.first[1]()
            down = push(self.axis, -1, h(after, 1), h(far, 1))
            self.last = [up, down]

        def near(self):
            for w in self.second:
                w()

        def end(self):
            for w in self.last:
                w()

    def pair(n):
        return lambda h: pl.ds(h * (n // 2), n // 2)

    rows = pair(vw.shape[-2])
    two = pair(N)
    own_v()
    v1 = direct("z", lambda i: vw.at[ci, yi, xi, i], lambda i, h: vw.at[ci, yi, xi, i, rows(h)])
    own_g()
    g1 = direct("y", lambda i: gw.at[ci, xi, zi, i], None)
    own_o()
    o1 = direct("x", lambda i: ow.at[ci, zi, yi, i], None)

    def wave(ref, w):
        off, count = waves[w]
        return lambda c, i: ref.at[c, i, :, :, pl.ds(off, count)]

    def wave_rings(w):
        off, count = waves[w]
        for ref, i in ((a_gu, xi), (b_gu, zi)):
            forward(fwd_gu[w], lambda c: wave(ref, w)(c, i))
        return (
            Ring("x", lambda i, h: a_gu.at[ci, i, two(h), :, pl.ds(off, count)]),
            Ring("z", lambda i, h: b_gu.at[ci, i, two(h), :, pl.ds(off, count)]),
        )

    def done(waits):
        for w in waits:
            w()

    def forward(keep, ref_of):
        keep.append(push("c", 1, ref_of(ci), ref_of(1 - ci)))

    def group(ref):
        return lambda c, i: ref.at[c, i]

    def finish_near(ring, keep, of, i):
        ring.near()
        forward(keep, lambda c: of(c, wrap(i, -1)))
        forward(keep, lambda c: of(c, wrap(i, 1)))

    def finish_far(ring, keep, of, i):
        ring.end()
        forward(keep, lambda c: of(c, wrap(i, 2)))

    fwd_v, fwd_g, fwd_o, fwd_gu = [], [], [], [[], [], []]
    done(own_gu)
    first = (Ring("z", lambda i, h: a_gu.at[ci, xi, i, h]),
             Ring("x", lambda i, h: b_gu.at[ci, zi, i, h]))
    done(v1)
    v2 = direct("x", lambda i: vw.at[ci, yi, i], None)
    done(g1)
    g2 = direct("z", lambda i: gw.at[ci, xi, i], lambda i, h: gw.at[ci, xi, i, two(h)])
    done(o1)
    o2 = direct("y", lambda i: ow.at[ci, zi, i], None)
    for ring in first:
        ring.relay()
    done(v2)
    v3 = Ring("y", lambda i, h: vw.at[ci, i, two(h)])
    forward(fwd_v, lambda c: vw.at[c, yi])
    done(g2)
    g3 = Ring("x", lambda i, h: gw.at[ci, i, two(h)])
    forward(fwd_g, lambda c: gw.at[c, xi])
    done(o2)
    o3 = Ring("z", lambda i, h: ow.at[ci, i, two(h)])
    forward(fwd_o, lambda c: ow.at[c, zi])

    got_tok()
    done(got_small)
    floats = tok[...].astype(F32)
    scale = lax.rsqrt(jnp.mean(floats * floats, axis=-1, keepdims=True) + EPS)
    nbuf[...] = (floats * scale * row(gain1)).astype(BF)

    v3.relay()
    g3.relay()
    o3.relay()
    for ring in first:
        ring.near()
        ring.end()
    second = [wave_rings(0), wave_rings(1)]
    finish_near(v3, fwd_v, group(vw), yi)
    finish_far(v3, fwd_v, group(vw), yi)
    finish_near(g3, fwd_g, group(gw), xi)
    finish_near(o3, fwd_o, group(ow), zi)
    done(fwd_v)

    every = [(z, x) for z in range(N) for x in range(N)]

    def project(block, lo):
        cols = [
            cat([block(c, y, z, x) for y in (lo, lo + 1) for c in range(2)], 0) for z, x in every
        ]
        return dot_nt(nbuf[...], cat(cols, 1))

    width = 512
    activated = gelu(cat([project(lambda c, y, z, x: vw[c, y, x, z], lo) for lo in (0, 2)], 1))
    center = jnp.sum(activated, axis=-1, keepdims=True) / width
    spread = jnp.sum(activated * activated, axis=-1, keepdims=True) / width - center * center
    values = (
        (activated - center) * lax.rsqrt(spread + EPS) * row(lgain) + row(lshift)
    ).astype(BF)
    finish_far(g3, fwd_g, group(gw), xi)
    finish_far(o3, fwd_o, group(ow), zi)
    span, groups = mixk.shape[1], mixk.shape[0]
    t_pos = lax.broadcasted_iota(jnp.int32, (span, span), 0)
    s_pos = lax.broadcasted_iota(jnp.int32, (span, span), 1)
    mixing = []
    for g in range(groups):
        masked = jnp.where(s_pos <= t_pos, mixk[g].astype(F32), 0.0).astype(BF)
        offset_row = mixo[g : g + 1, :].astype(F32)
        offset = jnp.sum(jnp.where(s_pos == t_pos, offset_row, 0.0), axis=-1, keepdims=True)
        mixing.append(
            jnp.dot(masked, values[:, g * span : (g + 1) * span], preferred_element_type=F32)
            + offset
        )
    done(fwd_g)
    gate_u = gelu(cat([project(lambda c, y, z, x: gw[c, x, z, y], lo) for lo in (0, 2)], 1))
    gated = (gate_u * cat(mixing, 1)).astype(BF)
    done(fwd_o)
    total = jnp.zeros((span, 1), F32)
    lane = 128
    for z in range(N):
        weights = cat(
            [
                cat([ow[c, z, y, x] for y in range(N) for c in range(2)], 0)
                for x in range(N)
            ],
            1,
        )
        cols = slice(z * N * lane, (z + 1) * N * lane)
        mid = (
            tok[:, cols].astype(F32) + jnp.dot(gated, weights, preferred_element_type=F32)
        ).astype(BF)
        middle[:, cols] = mid
        mid = mid.astype(F32)
        total += jnp.sum(mid * mid, axis=-1, keepdims=True)
    width2 = middle.shape[1]
    scale2 = lax.rsqrt(total / width2 + EPS)
    xall[yi] = (middle[...].astype(F32) * scale2 * row(gain2)).astype(BF)

    toks = Ring("y", lambda i, h: xall.at[i, pl.ds(h * (span // 2), span // 2)])

    order = [zi, wrap(zi, -1), wrap(zi, 1), wrap(zi, 2)]
    before, after, far = wrap(xi, -1), wrap(xi, 1), wrap(xi, 2)
    ad2, ad2_last = {}, {}

    def down_send(k):
        z = order[k]
        ad2[k] = [push("x", 1, a_d.at[ci, xi, z], a_d.at[ci, before, z]),
                  push("x", -1, a_d.at[ci, xi, z], a_d.at[ci, after, z])]

    def down_relay(k):
        z = order[k]
        ad2[k][0]()
        up = push("x", 1, a_d.at[ci, before, z, pl.ds(0, hr)], a_d.at[ci, far, z, pl.ds(0, hr)])
        ad2[k][1]()
        down = push(
            "x", -1, a_d.at[ci, after, z, pl.ds(hr, hr)], a_d.at[ci, far, z, pl.ds(hr, hr)]
        )
        ad2_last[k] = [up, down]

    def finish_wave(w):
        for finish in (finish_near, finish_far):
            finish(second[w][0], fwd_gu[w], wave(a_gu, w), xi)
            finish(second[w][1], fwd_gu[w], wave(b_gu, w), zi)

    for ring in second[0]:
        ring.relay()
    done(own_d)
    ad1 = Ring("z", lambda i, h: a_d.at[ci, xi, i, pl.ds(h * hr, hr)])
    bd1 = Ring("x", lambda i, h: b_d.at[ci, zi, i, pl.ds(h * hr, hr)])
    for ring in second[1]:
        ring.relay()
    second.append(wave_rings(2))
    toks.relay()
    finish_wave(0)
    for ring in (ad1, bd1):
        ring.relay()
    finish_wave(1)
    toks.near()
    done(fwd_gu[0])

    def unit_rows(w, which, lo, hi):
        count = waves[w][1]
        pieces = []
        for seg in range(4):
            a, b = max(lo, seg * count), min(hi, (seg + 1) * count)
            if a < b:
                c, h = divmod(seg, 2)
                r = slice(waves[w][0] + a - seg * count, waves[w][0] + b - seg * count)
                ref = (a_gu, b_gu)[h]
                pieces.append(
                    cat(
                        [
                            ref[(c, x, z) + (which, r)] if h == 0 else ref[(c, z, x) + (which, r)]
                            for z, x in every
                        ],
                        1,
                    )
                )
        return cat(pieces, 0)

    step = 256
    places = [yi, wrap(yi, -1), wrap(yi, 1), wrap(yi, 2)]

    def hidden_tile(w, lo, first, last):
        count = 4 * waves[w][1]
        hi = min(lo + step, count)
        block = cat([xall[y] for y in places[first:last]], 0)
        if hi - lo == step:
            gate_pre = dot_nt(block, unit_rows(w, 0, lo, hi))
            up_pre = dot_nt(block, unit_rows(w, 1, lo, hi))
        else:
            weights = cat([unit_rows(w, 0, lo, hi), unit_rows(w, 1, lo, hi)], 0)
            middle_row = block.shape[0] // 2
            both = cat([dot_nt(b, weights) for b in (block[:middle_row], block[middle_row:])], 0)
            gate_pre, up_pre = both[:, : hi - lo], both[:, hi - lo :]
        at = 4 * waves[w][0]
        hidden[first * span : last * span, at + lo : at + hi] = (
            gate_pre * lax.logistic(gate_pre) * up_pre
        ).astype(BF)

    hidden_tile(0, 0, 0, 3)
    hidden_tile(0, step, 0, 3)
    for ring in second[2]:
        ring.relay()
    down_send(0)
    done(fwd_gu[1])
    hidden_tile(1, 0, 0, 3)
    hidden_tile(1, step, 0, 3)
    for ring in (ad1, bd1):
        ring.near()
    down_send(1)
    for ring in (ad1, bd1):
        ring.end()
    bd2 = Ring("z", lambda i, h: b_d.at[ci, i, two(h)])
    fwd_d = [[] for _ in range(N + 1)]
    forward(fwd_d[0], lambda c: a_d.at[c, xi, zi])
    forward(fwd_d[0], lambda c: b_d.at[c, zi])
    toks.end()
    hidden_tile(0, 0, 3, 4)
    hidden_tile(0, step, 3, 4)
    finish_wave(2)
    hidden_tile(1, 0, 3, 4)
    hidden_tile(1, step, 3, 4)
    down_relay(0)
    down_send(2)
    forward(fwd_d[0], lambda c: a_d.at[c, wrap(xi, -1), zi])
    forward(fwd_d[1], lambda c: a_d.at[c, wrap(xi, 1), zi])
    done(fwd_gu[2])
    hidden_tile(2, 0, 0, 4)
    down_relay(1)
    down_send(3)
    bd2.relay()
    hidden_tile(2, step, 0, 4)

    def down_forward(k):
        z = order[k]
        done(ad2_last[k])
        forward(fwd_d[k + 1], lambda c: a_d.at[c, :, z])
        forward(fwd_d[k + 1], lambda c: b_d.at[c, z])

    got_r1, got_r2 = {}, {}
    own, back, ahead, opposite = range(N)

    pairs = (pl.ds(0, 2), pl.ds(2, 2))
    rounds = [
        (order[0], xi, before, (xi, before)),
        (order[0], after, far, (after, far)),
        (order[1], *pairs, range(N)),
        (order[2], *pairs, range(N)),
        (order[3], 0, 1, (0, 1)),
        (order[3], 2, 3, (2, 3)),
    ]

    def sum_first(r):
        z, low, high, _ = rounds[r]
        got_r1[r] = [
            send_to("y", 1, parts.at[opposite, z, low], r1.at[0, z, low]),
            send_to("y", -1, parts.at[opposite, z, high], r1.at[1, z, high]),
        ]

    def sum_direct(r):
        z, low, high, _ = rounds[r]
        got_r2[r] = [
            send_to("y", 1, parts.at[ahead, z, high], r2.at[0, z, high]),
            send_to("y", -1, parts.at[back, z, low], r2.at[1, z, low]),
        ]

    def send_to(axis, s, src, dst):
        k = len(sends)
        copy = pltpu.make_async_remote_copy(
            src, dst, ssem.at[k], rsem.at[k], device_id=device(axis, s),
            device_id_type=pl.DeviceIdType.MESH,
        )
        copy.start()
        sends.append(copy)
        return copy.wait_recv

    def sum_second(r):
        z, low, high, _ = rounds[r]
        got_r1[r][0]()
        parts[ahead, z, low] = (
            parts[ahead, z, low].astype(F32) + r1[0, z, low].astype(F32)
        ).astype(BF)
        got_r2[r].append(send_to("y", 1, parts.at[ahead, z, low], r2.at[0, z, low]))
        got_r1[r][1]()
        parts[back, z, high] = (
            parts[back, z, high].astype(F32) + r1[1, z, high].astype(F32)
        ).astype(BF)
        got_r2[r].append(send_to("y", -1, parts.at[back, z, high], r2.at[1, z, high]))

    def sum_last(r):
        z, _, _, blocks = rounds[r]
        done(got_r2[r])
        for x in blocks:
            summed = (
                parts[own, z, x].astype(F32) + r2[0, z, x].astype(F32) + r2[1, z, x].astype(F32)
            )
            cols = pl.ds(pl.multiple_of((z * N + x) * lane, lane), lane)
            out[:, cols] = (middle[:, cols].astype(F32) + summed).astype(BF)

    def multiply(z, xs):
        weights = cat(
            [
                cat(
                    [
                        ref
                        for off, count in waves
                        for c in range(2)
                        for ref in (a_d[c, x, z, off : off + count], b_d[c, z, x, off : off + count])
                    ],
                    0,
                )
                for x in xs
            ],
            1,
        )
        for y in range(0, N, 2):
            rows_y = hidden[y * span : (y + 2) * span, :]
            result = jnp.dot(rows_y, weights, preferred_element_type=F32).astype(BF)
            for i in range(2):
                for j, x in enumerate(xs):
                    parts[y + i, z, x] = result[
                        i * span : (i + 1) * span, j * lane : (j + 1) * lane
                    ]

    done(fwd_d[0])
    multiply(order[0], (xi, before))
    sum_first(0)
    sum_direct(0)
    done(ad2_last[0])
    forward(fwd_d[1], lambda c: a_d.at[c, wrap(xi, 2), zi])
    down_relay(2)
    bd2.near()
    down_forward(1)
    done(fwd_d[1])
    multiply(order[0], (after, far))
    sum_first(1)
    sum_direct(1)
    sum_second(0)
    done(fwd_d[2])
    multiply(order[1], (0, 1))
    multiply(order[1], (2, 3))
    sum_first(2)
    sum_direct(2)
    down_relay(3)
    down_forward(2)
    sum_second(1)
    done(fwd_d[3])
    multiply(order[2], (0, 1))
    multiply(order[2], (2, 3))
    sum_first(3)
    sum_direct(3)
    bd2.end()
    down_forward(3)
    sum_second(2)
    done(fwd_d[4])
    multiply(order[3], (0, 1))
    sum_first(4)
    multiply(order[3], (2, 3))
    sum_first(5)
    sum_direct(4)
    sum_direct(5)
    sum_second(3)
    sum_last(0)
    sum_last(1)
    sum_second(4)
    sum_second(5)
    sum_last(2)
    sum_last(3)
    sum_last(4)
    sum_last(5)
    assert len(sends) <= COPIES
    for copy in sends:
        copy.wait_send()


def per_device(
    tokens, mix_gain, gate_proj, value_proj, layer_gain, layer_shift, mix_kernel, mix_offset,
    out_proj, ffn_gain, ffn_gate, ffn_up, ffn_down,
):
    span, width = tokens.shape
    units, lane = ffn_gate.shape[1], ffn_gate.shape[0]
    local = gate_proj.shape[1]
    half = units // 2
    anywhere = pl.BlockSpec(memory_space=pl.ANY)
    return pl.pallas_call(
        kernel,
        out_shape=jax.ShapeDtypeStruct(tokens.shape, BF),
        in_specs=[anywhere] * 13,
        out_specs=pl.BlockSpec(memory_space=pltpu.VMEM),
        scratch_shapes=[
            pltpu.VMEM((span, width), BF),
            pltpu.VMEM(mix_gain.shape, BF),
            pltpu.VMEM(ffn_gain.shape, BF),
            pltpu.VMEM(layer_gain.shape, BF),
            pltpu.VMEM(layer_shift.shape, BF),
            pltpu.VMEM(mix_offset.shape, BF),
            pltpu.VMEM(mix_kernel.shape, BF),
            pltpu.VMEM((2, N, N, N, local, lane), BF),
            pltpu.VMEM((2, N, N, N, local, lane), BF),
            pltpu.VMEM((2, N, N, N, local, lane), BF),
            pltpu.VMEM((2, N, N, 2, half, lane), BF),
            pltpu.VMEM((2, N, N, 2, half, lane), BF),
            pltpu.VMEM((2, N, N, half, lane), BF),
            pltpu.VMEM((2, N, N, half, lane), BF),
            pltpu.VMEM((span, width), BF),
            pltpu.VMEM((span, width), BF),
            pltpu.VMEM((N, span, width), BF),
            pltpu.VMEM((N * span, 2 * units), BF),
            pltpu.VMEM((N, N, N, span, lane), BF),
            pltpu.VMEM((2, N, N, span, lane), BF),
            pltpu.VMEM((2, N, N, span, lane), BF),
            pltpu.SemaphoreType.DMA((24,)),
            pltpu.SemaphoreType.DMA((COPIES,)),
            pltpu.SemaphoreType.DMA((COPIES,)),
        ],
        compiler_params=pltpu.CompilerParams(
            collective_id=0, has_side_effects=True, vmem_limit_bytes=63 * 2**20
        ),
    )(
        tokens, gate_proj.T, value_proj.T, out_proj.T, ffn_gate.T, ffn_up.T, ffn_down.T,
        mix_gain, layer_gain, layer_shift, mix_kernel, mix_offset, ffn_gain,
    )


def solution(mesh):
    torus = Mesh(mesh.devices.reshape(mesh.shape["rep"], 4, 4, 4, 2), AXES)
    return jax.shard_map(
        per_device,
        mesh=torus,
        in_specs=(
            P(AXES, None), P(), P(FS, TP), P(FS, TP), P(), P(), P(), P(), P(FS, TP), P(),
            P(FS, TP), P(FS, TP), P(FS, TP),
        ),
        out_specs=P(AXES, None),
        check_vma=False,
    )
```

```python
import functools

import jax
import jax.numpy as jnp
from jax import lax
from jax.experimental import pallas as pl
from jax.experimental.pallas import tpu as pltpu
from jax.sharding import Mesh
from jax.sharding import PartitionSpec as P

AXES = ("rep", "fs_0", "fs_1", "tp_0", "tp_1")
FS = ("fs_0", "fs_1")
TP = ("tp_0", "tp_1")
EPS = 1e-06
N = 4
COPIES = 272


def row_waves(half):
    return [(0, 128), (128, 128), (256, half - 256)]

BF, F32 = jnp.bfloat16, jnp.float32


def dot_nt(left, right):
    return lax.dot_general(left, right, (((1,), (1,)), ((), ())), preferred_element_type=F32)


def gelu(v):
    return v * (0.5 * (1.0 + jnp.tanh(0.7978845608028654 * (v + 0.044715 * (v * v * v)))))


def row(ref):
    return ref[...].astype(F32).reshape(1, -1)


def cat(parts, axis):
    return jnp.concatenate(parts, axis=axis) if len(parts) > 1 else parts[0]


def kernel(
    tokens, gate_proj, value_proj, out_proj, ffn_gate, ffn_up, ffn_down, mix_gain, layer_gain,
    layer_shift, mix_kernel, mix_offset, ffn_gain,
    out,
    tok, gain1, gain2, lgain, lshift, mixo, mixk, vw, gw, ow, a_gu, b_gu, a_d, b_d, nbuf, middle, xall, hidden, parts, r1, r2,
    lsem, ssem, rsem,
):
    rep = lax.axis_index("rep")
    zi, xi, yi, ci = (lax.axis_index(a) for a in AXES[1:])

    def wrap(i, s):
        return lax.rem(i + (s + N), N)

    def device(axis, s):
        if axis == "z":
            z = lax.rem(rep * N + zi + (s + 2 * N), 2 * N)
            return {"rep": z // N, "fs_0": lax.rem(z, N)}
        if axis == "c":
            return {"tp_1": 1 - ci}
        name, i = {"x": ("fs_1", xi), "y": ("tp_0", yi)}[axis]
        return {name: wrap(i, s)}

    index = {"x": xi, "y": yi, "z": zi}
    sends = []

    def push(axis, s, mine, theirs):
        k = len(sends)
        to = device(axis, s)
        copy = pltpu.make_async_remote_copy(
            mine, mine, ssem.at[k], rsem.at[k], device_id=to, device_id_type=pl.DeviceIdType.MESH
        )
        copy.start()
        sends.append(copy)
        arrival = pltpu.make_async_remote_copy(
            theirs, theirs, ssem.at[k], rsem.at[k], device_id=to,
            device_id_type=pl.DeviceIdType.MESH,
        )
        return arrival.wait_recv

    locals_ = []

    def load(src, dst):
        copy = pltpu.make_async_copy(src, dst, lsem.at[len(locals_)])
        copy.start()
        locals_.append(copy)
        return copy.wait

    half = a_d.shape[-2]
    hr = half // 2
    waves = row_waves(half)
    own_v = load(value_proj, vw.at[ci, yi, xi, zi])
    own_g = load(gate_proj, gw.at[ci, xi, zi, yi])
    own_o = load(out_proj, ow.at[ci, zi, yi, xi])
    own_gu = [
        load(src.at[pl.ds(h * half, half)], dst.at[j])
        for h, dst in ((0, a_gu.at[ci, xi, zi]), (1, b_gu.at[ci, zi, xi]))
        for j, src in ((0, ffn_gate), (1, ffn_up))
    ]
    got_tok = load(tokens, tok)
    own_d = [
        load(ffn_down.at[pl.ds(0, half)], a_d.at[ci, xi, zi]),
        load(ffn_down.at[pl.ds(half, half)], b_d.at[ci, zi, xi]),
    ]
    got_small = [
        load(src, dst)
        for src, dst in (
            (mix_gain, gain1), (layer_gain, lgain), (layer_shift, lshift), (mix_kernel, mixk),
            (mix_offset, mixo), (ffn_gain, gain2),
        )
    ]

    barrier = pltpu.get_barrier_semaphore()
    greeted = [(a, s) for a in "xyz" for s in (1, -1, 2)] + [("z", -2), ("c", 1)]
    for a, s in greeted:
        pl.semaphore_signal(
            barrier, inc=1, device_id=device(a, s), device_id_type=pl.DeviceIdType.MESH
        )
    pl.semaphore_wait(barrier, len(greeted))

    def direct(axis, group, halves):
        i = index[axis]
        got = [
            push(axis, 1, group(i), group(wrap(i, -1))),
            push(axis, -1, group(i), group(wrap(i, 1))),
        ]
        far = wrap(i, 2)
        if axis == "z":
            got += [push(axis, 2, halves(i, 0), halves(far, 0)),
                    push(axis, -2, halves(i, 1), halves(far, 1))]
        else:
            got += [push(axis, 2, group(i), group(far))]
        return got

    class Ring:
        def __init__(self, axis, halves):
            self.axis, self.halves, self.i = axis, halves, index[axis]
            i = self.i
            before, after = wrap(i, -1), wrap(i, 1)
            self.first = [push(axis, 1, halves(i, 0), halves(before, 0)),
                          push(axis, -1, halves(i, 1), halves(after, 1))]
            self.second = [push(axis, 1, halves(i, 1), halves(before, 1)),
                           push(axis, -1, halves(i, 0), halves(after, 0))]

        def relay(self):
            i, h = self.i, self.halves
            before, after, far = wrap(i, -1), wrap(i, 1), wrap(i, 2)
            self.first[0]()
            up = push(self.axis, 1, h(before, 0), h(far, 0))
            self.first[1]()
            down = push(self.axis, -1, h(after, 1), h(far, 1))
            self.last = [up, down]

        def near(self):
            for w in self.second:
                w()

        def end(self):
            for w in self.last:
                w()

    def pair(n):
        return lambda h: pl.ds(h * (n // 2), n // 2)

    rows = pair(vw.shape[-2])
    two = pair(N)
    own_v()
    v1 = direct("z", lambda i: vw.at[ci, yi, xi, i], lambda i, h: vw.at[ci, yi, xi, i, rows(h)])
    own_g()
    g1 = direct("y", lambda i: gw.at[ci, xi, zi, i], None)
    own_o()
    o1 = direct("x", lambda i: ow.at[ci, zi, yi, i], None)

    def wave(ref, w):
        off, count = waves[w]
        return lambda c, i: ref.at[c, i, :, :, pl.ds(off, count)]

    def wave_rings(w):
        off, count = waves[w]
        for ref, i in ((a_gu, xi), (b_gu, zi)):
            forward(fwd_gu[w], lambda c: wave(ref, w)(c, i))
        return (
            Ring("x", lambda i, h: a_gu.at[ci, i, two(h), :, pl.ds(off, count)]),
            Ring("z", lambda i, h: b_gu.at[ci, i, two(h), :, pl.ds(off, count)]),
        )

    def done(waits):
        for w in waits:
            w()

    def forward(keep, ref_of):
        keep.append(push("c", 1, ref_of(ci), ref_of(1 - ci)))

    def group(ref):
        return lambda c, i: ref.at[c, i]

    def finish_near(ring, keep, of, i):
        ring.near()
        forward(keep, lambda c: of(c, wrap(i, -1)))
        forward(keep, lambda c: of(c, wrap(i, 1)))

    def finish_far(ring, keep, of, i):
        ring.end()
        forward(keep, lambda c: of(c, wrap(i, 2)))

    fwd_v, fwd_g, fwd_o, fwd_gu = [], [], [], [[], [], []]
    done(own_gu)
    first = (Ring("z", lambda i, h: a_gu.at[ci, xi, i, h]),
             Ring("x", lambda i, h: b_gu.at[ci, zi, i, h]))
    done(v1)
    v2 = direct("x", lambda i: vw.at[ci, yi, i], None)
    done(g1)
    g2 = direct("z", lambda i: gw.at[ci, xi, i], lambda i, h: gw.at[ci, xi, i, two(h)])
    done(o1)
    o2 = direct("y", lambda i: ow.at[ci, zi, i], None)
    for ring in first:
        ring.relay()
    done(v2)
    v3 = Ring("y", lambda i, h: vw.at[ci, i, two(h)])
    forward(fwd_v, lambda c: vw.at[c, yi])
    done(g2)
    g3 = Ring("x", lambda i, h: gw.at[ci, i, two(h)])
    forward(fwd_g, lambda c: gw.at[c, xi])
    done(o2)
    o3 = Ring("z", lambda i, h: ow.at[ci, i, two(h)])
    forward(fwd_o, lambda c: ow.at[c, zi])

    got_tok()
    done(got_small)
    floats = tok[...].astype(F32)
    scale = lax.rsqrt(jnp.mean(floats * floats, axis=-1, keepdims=True) + EPS)
    nbuf[...] = (floats * scale * row(gain1)).astype(BF)

    v3.relay()
    g3.relay()
    o3.relay()
    for ring in first:
        ring.near()
        ring.end()
    second = [wave_rings(0), wave_rings(1)]
    finish_near(v3, fwd_v, group(vw), yi)
    finish_far(v3, fwd_v, group(vw), yi)
    finish_near(g3, fwd_g, group(gw), xi)
    finish_near(o3, fwd_o, group(ow), zi)
    done(fwd_v)

    every = [(z, x) for z in range(N) for x in range(N)]

    def project(block, lo):
        cols = [
            cat([block(c, y, z, x) for y in (lo, lo + 1) for c in range(2)], 0) for z, x in every
        ]
        return dot_nt(nbuf[...], cat(cols, 1))

    width = 512
    activated = gelu(cat([project(lambda c, y, z, x: vw[c, y, x, z], lo) for lo in (0, 2)], 1))
    center = jnp.sum(activated, axis=-1, keepdims=True) / width
    spread = jnp.sum(activated * activated, axis=-1, keepdims=True) / width - center * center
    values = (
        (activated - center) * lax.rsqrt(spread + EPS) * row(lgain) + row(lshift)
    ).astype(BF)
    finish_far(g3, fwd_g, group(gw), xi)
    finish_far(o3, fwd_o, group(ow), zi)
    span, groups = mixk.shape[1], mixk.shape[0]
    t_pos = lax.broadcasted_iota(jnp.int32, (span, span), 0)
    s_pos = lax.broadcasted_iota(jnp.int32, (span, span), 1)
    mixing = []
    for g in range(groups):
        masked = jnp.where(s_pos <= t_pos, mixk[g].astype(F32), 0.0).astype(BF)
        offset_row = mixo[g : g + 1, :].astype(F32)
        offset = jnp.sum(jnp.where(s_pos == t_pos, offset_row, 0.0), axis=-1, keepdims=True)
        mixing.append(
            jnp.dot(masked, values[:, g * span : (g + 1) * span], preferred_element_type=F32)
            + offset
        )
    done(fwd_g)
    gate_u = gelu(cat([project(lambda c, y, z, x: gw[c, x, z, y], lo) for lo in (0, 2)], 1))
    gated = (gate_u * cat(mixing, 1)).astype(BF)
    done(fwd_o)
    total = jnp.zeros((span, 1), F32)
    lane = 128
    for z in range(N):
        weights = cat(
            [
                cat([ow[c, z, y, x] for y in range(N) for c in range(2)], 0)
                for x in range(N)
            ],
            1,
        )
        cols = slice(z * N * lane, (z + 1) * N * lane)
        mid = (
            tok[:, cols].astype(F32) + jnp.dot(gated, weights, preferred_element_type=F32)
        ).astype(BF)
        middle[:, cols] = mid
        mid = mid.astype(F32)
        total += jnp.sum(mid * mid, axis=-1, keepdims=True)
    width2 = middle.shape[1]
    scale2 = lax.rsqrt(total / width2 + EPS)
    xall[yi] = (middle[...].astype(F32) * scale2 * row(gain2)).astype(BF)

    toks = Ring("y", lambda i, h: xall.at[i, pl.ds(h * (span // 2), span // 2)])

    places_x = [xi, wrap(xi, -1), wrap(xi, 1), wrap(xi, 2)]
    places_z = [zi, wrap(zi, -1), wrap(zi, 1), wrap(zi, 2)]
    got_near, got_far = {}, {}
    fwd_d = [[] for _ in range(8)]

    def block_a(c, x, z, at=pl.ds(0, half)):
        return a_d.at[c, x, z, at]

    def block_b(c, z, x, at=pl.ds(0, half)):
        return b_d.at[c, z, x, at]

    lines = (("x", block_a, places_x, places_z), ("z", block_b, places_z, places_x))

    def down_send(k):
        for axis, block, along, other in lines:
            mine = block(ci, along[0], other[k])
            got_near[axis, k] = [push(axis, 1, mine, block(ci, along[1], other[k])),
                                 push(axis, -1, mine, block(ci, along[2], other[k]))]

    def down_near(k):
        for axis, block, along, other in lines:
            got_far[axis, k] = []
            for h, (w, s, j) in enumerate(zip(got_near[axis, k], (1, -1), (1, 2))):
                w()
                at = pl.ds(h * hr, hr)
                got_far[axis, k].append(
                    push(axis, s, block(ci, along[j], other[k], at), block(ci, along[3], other[k], at))
                )

    def down_near_forward(f, k):
        for axis, block, along, other in lines:
            for j in (1, 2):
                forward(fwd_d[f], lambda c: block(c, along[j], other[k]))

    def down_far_forward(f, k):
        for axis, block, along, other in lines:
            done(got_far[axis, k])
            forward(fwd_d[f], lambda c: block(c, along[3], other[k]))

    def near_wave(w):
        finish_near(second[w][0], fwd_gu[w], wave(a_gu, w), xi)
        finish_near(second[w][1], fwd_gu[w], wave(b_gu, w), zi)

    def far_wave(w):
        finish_far(second[w][0], fwd_gu[w], wave(a_gu, w), xi)
        finish_far(second[w][1], fwd_gu[w], wave(b_gu, w), zi)

    for ring in second[0]:
        ring.relay()
    done(own_d)
    ad1 = Ring("z", lambda i, h: a_d.at[ci, xi, i, pl.ds(h * hr, hr)])
    bd1 = Ring("x", lambda i, h: b_d.at[ci, zi, i, pl.ds(h * hr, hr)])
    for ring in second[1]:
        ring.relay()
    second.append(wave_rings(2))
    near_wave(0)
    toks.relay()
    far_wave(0)
    for ring in (ad1, bd1):
        ring.relay()
    near_wave(1)
    toks.near()
    done(fwd_gu[0])

    def unit_rows(w, which, lo, hi):
        count = waves[w][1]
        pieces = []
        for seg in range(4):
            a, b = max(lo, seg * count), min(hi, (seg + 1) * count)
            if a < b:
                c, h = divmod(seg, 2)
                r = slice(waves[w][0] + a - seg * count, waves[w][0] + b - seg * count)
                ref = (a_gu, b_gu)[h]
                pieces.append(
                    cat(
                        [
                            ref[(c, x, z) + (which, r)] if h == 0 else ref[(c, z, x) + (which, r)]
                            for z, x in every
                        ],
                        1,
                    )
                )
        return cat(pieces, 0)

    step = 256
    places = [yi, wrap(yi, -1), wrap(yi, 1), wrap(yi, 2)]

    def hidden_tile(w, lo, first, last):
        count = 4 * waves[w][1]
        hi = min(lo + step, count)
        block = cat([xall[y] for y in places[first:last]], 0)
        if hi - lo == step:
            gate_pre = dot_nt(block, unit_rows(w, 0, lo, hi))
            up_pre = dot_nt(block, unit_rows(w, 1, lo, hi))
        else:
            weights = cat([unit_rows(w, 0, lo, hi), unit_rows(w, 1, lo, hi)], 0)
            middle_row = block.shape[0] // 2
            both = cat([dot_nt(b, weights) for b in (block[:middle_row], block[middle_row:])], 0)
            gate_pre, up_pre = both[:, : hi - lo], both[:, hi - lo :]
        at = 4 * waves[w][0]
        hidden[first * span : last * span, at + lo : at + hi] = (
            gate_pre * lax.logistic(gate_pre) * up_pre
        ).astype(BF)

    hidden_tile(0, 0, 0, 3)
    hidden_tile(0, step, 0, 3)
    far_wave(1)
    for ring in second[2]:
        ring.relay()
    down_send(0)
    done(fwd_gu[1])
    hidden_tile(1, 0, 0, 3)
    hidden_tile(1, step, 0, 3)
    near_wave(2)
    for ring in (ad1, bd1):
        ring.near()
    down_send(1)
    down_send(2)
    for ring in (ad1, bd1):
        ring.end()
    forward(fwd_d[0], lambda c: a_d.at[c, xi])
    forward(fwd_d[0], lambda c: b_d.at[c, zi])
    toks.end()
    hidden_tile(0, 0, 3, 4)
    hidden_tile(0, step, 3, 4)
    far_wave(2)
    hidden_tile(1, 0, 3, 4)
    hidden_tile(1, step, 3, 4)
    down_near(0)
    down_near_forward(1, 0)
    down_send(3)
    done(fwd_gu[2])
    hidden_tile(2, 0, 0, 4)
    hidden_tile(2, step, 0, 4)

    got_r1, got_r2 = {}, {}
    own, back, ahead, opposite = range(N)

    order = [(0, 0), (0, 1), (1, 0), (2, 0), (0, 2), (1, 1), (1, 2), (2, 1), (2, 2), (0, 3), (3, 0),
             (1, 3), (2, 3), (3, 1), (3, 2), (3, 3)]
    blocks = [(places_z[i], places_x[j]) for i, j in order]
    rounds = [(blocks[r], blocks[r + 1]) for r in range(0, len(blocks), 2)]

    def sum_first(r):
        low, high = rounds[r]
        got_r1[r] = [
            send_to("y", 1, parts.at[(opposite, *low)], r1.at[(0, *low)]),
            send_to("y", -1, parts.at[(opposite, *high)], r1.at[(1, *high)]),
        ]

    def sum_direct(r):
        low, high = rounds[r]
        got_r2[r] = [
            send_to("y", 1, parts.at[(ahead, *high)], r2.at[(0, *high)]),
            send_to("y", -1, parts.at[(back, *low)], r2.at[(1, *low)]),
        ]

    def send_to(axis, s, src, dst):
        k = len(sends)
        copy = pltpu.make_async_remote_copy(
            src, dst, ssem.at[k], rsem.at[k], device_id=device(axis, s),
            device_id_type=pl.DeviceIdType.MESH,
        )
        copy.start()
        sends.append(copy)
        return copy.wait_recv

    def sum_second(r):
        for k, (s, rel, at) in enumerate(((1, ahead, rounds[r][0]), (-1, back, rounds[r][1]))):
            got_r1[r][k]()
            parts[(rel, *at)] = (
                parts[(rel, *at)].astype(F32) + r1[(k, *at)].astype(F32)
            ).astype(BF)
            got_r2[r].append(send_to("y", s, parts.at[(rel, *at)], r2.at[(k, *at)]))

    def sum_last(r):
        done(got_r2[r])
        for z, x in rounds[r]:
            summed = (
                parts[own, z, x].astype(F32) + r2[0, z, x].astype(F32) + r2[1, z, x].astype(F32)
            )
            cols = pl.ds(pl.multiple_of((z * N + x) * lane, lane), lane)
            out[:, cols] = (middle[:, cols].astype(F32) + summed).astype(BF)

    def multiply(r):
        weights = cat(
            [
                cat(
                    [
                        ref
                        for off, count in waves
                        for c in range(2)
                        for ref in (a_d[c, x, z, off : off + count], b_d[c, z, x, off : off + count])
                    ],
                    0,
                )
                for z, x in rounds[r]
            ],
            1,
        )
        for y in range(0, N, 2):
            rows_y = hidden[y * span : (y + 2) * span, :]
            result = jnp.dot(rows_y, weights, preferred_element_type=F32).astype(BF)
            for i in range(2):
                for j, (z, x) in enumerate(rounds[r]):
                    parts[y + i, z, x] = result[
                        i * span : (i + 1) * span, j * lane : (j + 1) * lane
                    ]

    done(fwd_d[0])
    done(fwd_d[1])
    multiply(0)
    sum_first(0)
    multiply(1)
    sum_first(1)
    sum_direct(0)
    sum_direct(1)
    down_near(1)
    down_near_forward(2, 1)
    down_near(2)
    down_near_forward(3, 2)
    done(fwd_d[2])
    multiply(2)
    sum_first(2)
    sum_direct(2)
    down_far_forward(4, 0)
    done(fwd_d[3])
    multiply(3)
    sum_first(3)
    sum_second(0)
    sum_second(1)
    sum_direct(3)
    done(fwd_d[4])
    multiply(4)
    sum_first(4)
    down_near(3)
    down_near_forward(5, 3)
    sum_second(2)
    sum_direct(4)
    down_far_forward(6, 1)
    down_far_forward(6, 2)
    sum_second(3)
    done(fwd_d[5])
    done(fwd_d[6])
    multiply(5)
    sum_first(5)
    multiply(6)
    sum_first(6)
    sum_direct(5)
    down_far_forward(7, 3)
    sum_second(4)
    done(fwd_d[7])
    multiply(7)
    sum_first(7)
    sum_direct(6)
    sum_direct(7)
    sum_last(0)
    sum_last(1)
    sum_second(5)
    sum_second(6)
    sum_last(2)
    sum_last(3)
    sum_second(7)
    sum_last(4)
    sum_last(5)
    sum_last(6)
    sum_last(7)
    assert len(sends) <= COPIES
    for copy in sends:
        copy.wait_send()


def per_device(
    tokens, mix_gain, gate_proj, value_proj, layer_gain, layer_shift, mix_kernel, mix_offset,
    out_proj, ffn_gain, ffn_gate, ffn_up, ffn_down,
):
    span, width = tokens.shape
    units, lane = ffn_gate.shape[1], ffn_gate.shape[0]
    local = gate_proj.shape[1]
    half = units // 2
    anywhere = pl.BlockSpec(memory_space=pl.ANY)
    return pl.pallas_call(
        kernel,
        out_shape=pltpu.VMEM(tokens.shape, BF),
        in_specs=[anywhere] * 13,
        out_specs=pl.BlockSpec(memory_space=pltpu.VMEM),
        scratch_shapes=[
            pltpu.VMEM((span, width), BF),
            pltpu.VMEM(mix_gain.shape, BF),
            pltpu.VMEM(ffn_gain.shape, BF),
            pltpu.VMEM(layer_gain.shape, BF),
            pltpu.VMEM(layer_shift.shape, BF),
            pltpu.VMEM(mix_offset.shape, BF),
            pltpu.VMEM(mix_kernel.shape, BF),
            pltpu.VMEM((2, N, N, N, local, lane), BF),
            pltpu.VMEM((2, N, N, N, local, lane), BF),
            pltpu.VMEM((2, N, N, N, local, lane), BF),
            pltpu.VMEM((2, N, N, 2, half, lane), BF),
            pltpu.VMEM((2, N, N, 2, half, lane), BF),
            pltpu.VMEM((2, N, N, half, lane), BF),
            pltpu.VMEM((2, N, N, half, lane), BF),
            pltpu.VMEM((span, width), BF),
            pltpu.VMEM((span, width), BF),
            pltpu.VMEM((N, span, width), BF),
            pltpu.VMEM((N * span, 2 * units), BF),
            pltpu.VMEM((N, N, N, span, lane), BF),
            pltpu.VMEM((2, N, N, span, lane), BF),
            pltpu.VMEM((2, N, N, span, lane), BF),
            pltpu.SemaphoreType.DMA((24,)),
            pltpu.SemaphoreType.DMA((COPIES,)),
            pltpu.SemaphoreType.DMA((COPIES,)),
        ],
        compiler_params=pltpu.CompilerParams(
            collective_id=0, has_side_effects=True, vmem_limit_bytes=63 * 2**20
        ),
    )(
        tokens, gate_proj.T, value_proj.T, out_proj.T, ffn_gate.T, ffn_up.T, ffn_down.T,
        mix_gain, layer_gain, layer_shift, mix_kernel, mix_offset, ffn_gain,
    )


def solution(mesh):
    torus = Mesh(mesh.devices.reshape(mesh.shape["rep"], 4, 4, 4, 2), AXES)
    return jax.shard_map(
        per_device,
        mesh=torus,
        in_specs=(
            P(AXES, None), P(), P(FS, TP), P(FS, TP), P(), P(), P(), P(), P(FS, TP), P(),
            P(FS, TP), P(FS, TP), P(FS, TP),
        ),
        out_specs=P(AXES, None),
        check_vma=False,
    )
```

```python
import functools

import jax
import jax.numpy as jnp
from jax import lax
from jax.experimental import pallas as pl
from jax.experimental.pallas import tpu as pltpu
from jax.sharding import Mesh
from jax.sharding import PartitionSpec as P

AXES = ("rep", "fs_0", "fs_1", "tp_0", "tp_1")
FS = ("fs_0", "fs_1")
TP = ("tp_0", "tp_1")
EPS = 1e-06
N = 4
COPIES = 280


def row_waves(half):
    return [(0, 128), (128, 128), (256, half - 256)]

BF, F32 = jnp.bfloat16, jnp.float32


def dot_nt(left, right):
    return lax.dot_general(left, right, (((1,), (1,)), ((), ())), preferred_element_type=F32)


def gelu(v):
    return v * (0.5 * (1.0 + jnp.tanh(0.7978845608028654 * (v + 0.044715 * (v * v * v)))))


def row(ref):
    return ref[...].astype(F32).reshape(1, -1)


def cat(parts, axis):
    return jnp.concatenate(parts, axis=axis) if len(parts) > 1 else parts[0]


def kernel(
    tokens, gate_proj, value_proj, out_proj, ffn_gate, ffn_up, ffn_down, mix_gain, layer_gain,
    layer_shift, mix_kernel, mix_offset, ffn_gain,
    out,
    tok, gain1, gain2, lgain, lshift, mixo, mixk, vw, gw, ow, a_gu, b_gu, a_d, b_d, nbuf, middle, xall, hidden, parts, r1, r2,
    lsem, ssem, rsem,
):
    rep = lax.axis_index("rep")
    zi, xi, yi, ci = (lax.axis_index(a) for a in AXES[1:])

    def wrap(i, s):
        return lax.rem(i + (s + N), N)

    def device(axis, s):
        if axis == "z":
            z = lax.rem(rep * N + zi + (s + 2 * N), 2 * N)
            return {"rep": z // N, "fs_0": lax.rem(z, N)}
        if axis == "c":
            return {"tp_1": 1 - ci}
        name, i = {"x": ("fs_1", xi), "y": ("tp_0", yi)}[axis]
        return {name: wrap(i, s)}

    index = {"x": xi, "y": yi, "z": zi}
    sends = []

    def push(axis, s, mine, theirs):
        k = len(sends)
        to = device(axis, s)
        copy = pltpu.make_async_remote_copy(
            mine, mine, ssem.at[k], rsem.at[k], device_id=to, device_id_type=pl.DeviceIdType.MESH
        )
        copy.start()
        sends.append(copy)
        arrival = pltpu.make_async_remote_copy(
            theirs, theirs, ssem.at[k], rsem.at[k], device_id=to,
            device_id_type=pl.DeviceIdType.MESH,
        )
        return arrival.wait_recv

    locals_ = []

    def load(src, dst):
        copy = pltpu.make_async_copy(src, dst, lsem.at[len(locals_)])
        copy.start()
        locals_.append(copy)
        return copy.wait

    half = a_d.shape[-2]
    hr = half // 2
    waves = row_waves(half)
    own_v = load(value_proj, vw.at[ci, yi, xi, zi])
    own_g = load(gate_proj, gw.at[ci, xi, zi, yi])
    own_o = load(out_proj, ow.at[ci, zi, yi, xi])
    own_gu = [
        load(src.at[pl.ds(h * half, half)], dst.at[j])
        for h, dst in ((0, a_gu.at[ci, xi, zi]), (1, b_gu.at[ci, zi, xi]))
        for j, src in ((0, ffn_gate), (1, ffn_up))
    ]
    got_tok = load(tokens, tok)
    own_d = [
        load(ffn_down.at[pl.ds(0, half)], a_d.at[ci, xi, zi]),
        load(ffn_down.at[pl.ds(half, half)], b_d.at[ci, zi, xi]),
    ]
    got_small = [
        load(src, dst)
        for src, dst in (
            (mix_gain, gain1), (layer_gain, lgain), (layer_shift, lshift), (mix_kernel, mixk),
            (mix_offset, mixo), (ffn_gain, gain2),
        )
    ]

    barrier = pltpu.get_barrier_semaphore()
    greeted = [(a, s) for a in "xyz" for s in (1, -1, 2)] + [("z", -2), ("c", 1)]
    for a, s in greeted:
        pl.semaphore_signal(
            barrier, inc=1, device_id=device(a, s), device_id_type=pl.DeviceIdType.MESH
        )
    pl.semaphore_wait(barrier, len(greeted))

    def direct(axis, group, halves):
        i = index[axis]
        got = [
            push(axis, 1, group(i), group(wrap(i, -1))),
            push(axis, -1, group(i), group(wrap(i, 1))),
        ]
        far = wrap(i, 2)
        if axis == "z":
            got += [push(axis, 2, halves(i, 0), halves(far, 0)),
                    push(axis, -2, halves(i, 1), halves(far, 1))]
        else:
            got += [push(axis, 2, group(i), group(far))]
        return got

    class Ring:
        def __init__(self, axis, halves):
            self.axis, self.halves, self.i = axis, halves, index[axis]
            i = self.i
            before, after = wrap(i, -1), wrap(i, 1)
            self.first = [push(axis, 1, halves(i, 0), halves(before, 0)),
                          push(axis, -1, halves(i, 1), halves(after, 1))]
            self.second = [push(axis, 1, halves(i, 1), halves(before, 1)),
                           push(axis, -1, halves(i, 0), halves(after, 0))]

        def relay(self):
            i, h = self.i, self.halves
            before, after, far = wrap(i, -1), wrap(i, 1), wrap(i, 2)
            self.first[0]()
            up = push(self.axis, 1, h(before, 0), h(far, 0))
            self.first[1]()
            down = push(self.axis, -1, h(after, 1), h(far, 1))
            self.last = [up, down]

        def near(self):
            for w in self.second:
                w()

        def end(self):
            for w in self.last:
                w()

    def pair(n):
        return lambda h: pl.ds(h * (n // 2), n // 2)

    rows = pair(vw.shape[-2])
    two = pair(N)
    own_v()
    v1 = direct("z", lambda i: vw.at[ci, yi, xi, i], lambda i, h: vw.at[ci, yi, xi, i, rows(h)])
    own_g()
    g1 = direct("y", lambda i: gw.at[ci, xi, zi, i], None)
    own_o()
    o1 = direct("x", lambda i: ow.at[ci, zi, yi, i], None)

    def wave(ref, w):
        off, count = waves[w]
        return lambda c, i: ref.at[c, i, :, :, pl.ds(off, count)]

    def wave_rings(w):
        off, count = waves[w]
        for ref, i in ((a_gu, xi), (b_gu, zi)):
            forward(fwd_gu[w], lambda c: wave(ref, w)(c, i))
        return (
            Ring("x", lambda i, h: a_gu.at[ci, i, two(h), :, pl.ds(off, count)]),
            Ring("z", lambda i, h: b_gu.at[ci, i, two(h), :, pl.ds(off, count)]),
        )

    def done(waits):
        for w in waits:
            w()

    def forward(keep, ref_of):
        keep.append(push("c", 1, ref_of(ci), ref_of(1 - ci)))

    def group(ref):
        return lambda c, i: ref.at[c, i]

    def finish_near(ring, keep, of, i):
        ring.near()
        forward(keep, lambda c: of(c, wrap(i, -1)))
        forward(keep, lambda c: of(c, wrap(i, 1)))

    def finish_far(ring, keep, of, i):
        ring.end()
        forward(keep, lambda c: of(c, wrap(i, 2)))

    fwd_v, fwd_g, fwd_o, fwd_gu = [], [], [], [[], [], []]
    done(own_gu)
    first = (Ring("z", lambda i, h: a_gu.at[ci, xi, i, h]),
             Ring("x", lambda i, h: b_gu.at[ci, zi, i, h]))
    done(v1)
    v2 = direct("x", lambda i: vw.at[ci, yi, i], None)
    done(g1)
    g2 = direct("z", lambda i: gw.at[ci, xi, i], lambda i, h: gw.at[ci, xi, i, two(h)])
    done(o1)
    o2 = direct("y", lambda i: ow.at[ci, zi, i], None)
    for ring in first:
        ring.relay()
    done(v2)
    v3 = Ring("y", lambda i, h: vw.at[ci, i, two(h)])
    forward(fwd_v, lambda c: vw.at[c, yi])
    done(g2)
    g3 = Ring("x", lambda i, h: gw.at[ci, i, two(h)])
    forward(fwd_g, lambda c: gw.at[c, xi])
    done(o2)
    o3 = Ring("z", lambda i, h: ow.at[ci, i, two(h)])
    forward(fwd_o, lambda c: ow.at[c, zi])

    got_tok()
    done(got_small)
    floats = tok[...].astype(F32)
    scale = lax.rsqrt(jnp.mean(floats * floats, axis=-1, keepdims=True) + EPS)
    nbuf[...] = (floats * scale * row(gain1)).astype(BF)

    v3.relay()
    g3.relay()
    o3.relay()
    for ring in first:
        ring.near()
        ring.end()
    second = [wave_rings(0), wave_rings(1)]
    finish_near(v3, fwd_v, group(vw), yi)
    finish_far(v3, fwd_v, group(vw), yi)
    finish_near(g3, fwd_g, group(gw), xi)
    finish_near(o3, fwd_o, group(ow), zi)
    done(fwd_v)

    every = [(z, x) for z in range(N) for x in range(N)]

    def project(block, lo):
        cols = [
            cat([block(c, y, z, x) for y in (lo, lo + 1) for c in range(2)], 0) for z, x in every
        ]
        return dot_nt(nbuf[...], cat(cols, 1))

    width = 512
    activated = gelu(cat([project(lambda c, y, z, x: vw[c, y, x, z], lo) for lo in (0, 2)], 1))
    center = jnp.sum(activated, axis=-1, keepdims=True) / width
    spread = jnp.sum(activated * activated, axis=-1, keepdims=True) / width - center * center
    values = (
        (activated - center) * lax.rsqrt(spread + EPS) * row(lgain) + row(lshift)
    ).astype(BF)
    done(fwd_g[:3])
    ring_x = [xi, wrap(xi, -1), wrap(xi, 1), wrap(xi, 2)]

    def gate_part(xs):
        pairs = [(z, x) for z in range(N) for x in xs]
        left = cat(
            [nbuf[:, pl.ds(pl.multiple_of((z * N + x) * 128, 128), 128)] for z, x in pairs], 1
        )
        return cat(
            [
                dot_nt(
                    left,
                    cat(
                        [
                            cat([gw[c, x, z, y] for y in (lo, lo + 1) for c in range(2)], 0)
                            for z, x in pairs
                        ],
                        1,
                    ),
                )
                for lo in (0, 2)
            ],
            1,
        )

    gate_near = gate_part(ring_x[:3])
    finish_far(g3, fwd_g, group(gw), xi)
    finish_far(o3, fwd_o, group(ow), zi)
    span, groups = mixk.shape[1], mixk.shape[0]
    t_pos = lax.broadcasted_iota(jnp.int32, (span, span), 0)
    s_pos = lax.broadcasted_iota(jnp.int32, (span, span), 1)
    mixing = []
    for g in range(groups):
        masked = jnp.where(s_pos <= t_pos, mixk[g].astype(F32), 0.0).astype(BF)
        offset_row = mixo[g : g + 1, :].astype(F32)
        offset = jnp.sum(jnp.where(s_pos == t_pos, offset_row, 0.0), axis=-1, keepdims=True)
        mixing.append(
            jnp.dot(masked, values[:, g * span : (g + 1) * span], preferred_element_type=F32)
            + offset
        )
    done(fwd_g[3:])
    gate_u = gelu(gate_near + gate_part(ring_x[3:]))
    gated = (gate_u * cat(mixing, 1)).astype(BF)
    done(fwd_o)
    total = jnp.zeros((span, 1), F32)
    lane = 128
    for z in range(N):
        weights = cat(
            [
                cat([ow[c, z, y, x] for y in range(N) for c in range(2)], 0)
                for x in range(N)
            ],
            1,
        )
        cols = slice(z * N * lane, (z + 1) * N * lane)
        mid = (
            tok[:, cols].astype(F32) + jnp.dot(gated, weights, preferred_element_type=F32)
        ).astype(BF)
        middle[:, cols] = mid
        mid = mid.astype(F32)
        total += jnp.sum(mid * mid, axis=-1, keepdims=True)
    width2 = middle.shape[1]
    scale2 = lax.rsqrt(total / width2 + EPS)
    xall[yi] = (middle[...].astype(F32) * scale2 * row(gain2)).astype(BF)

    toks = Ring("y", lambda i, h: xall.at[i, pl.ds(h * (span // 2), span // 2)])

    places_x = [xi, wrap(xi, -1), wrap(xi, 1), wrap(xi, 2)]
    places_z = [zi, wrap(zi, -1), wrap(zi, 1), wrap(zi, 2)]
    got_near, got_far = {}, {}
    fwd_d = [[] for _ in range(8)]

    def block_a(c, x, z, at=pl.ds(0, half)):
        return a_d.at[c, x, z, at]

    def block_b(c, z, x, at=pl.ds(0, half)):
        return b_d.at[c, z, x, at]

    lines = (("x", block_a, places_x, places_z), ("z", block_b, places_z, places_x))

    def down_send(k):
        for axis, block, along, other in lines:
            mine = block(ci, along[0], other[k])
            got_near[axis, k] = [push(axis, 1, mine, block(ci, along[1], other[k])),
                                 push(axis, -1, mine, block(ci, along[2], other[k]))]

    def down_near(k):
        for axis, block, along, other in lines:
            got_far[axis, k] = []
            for h, (w, s, j) in enumerate(zip(got_near[axis, k], (1, -1), (1, 2))):
                w()
                at = pl.ds(h * hr, hr)
                got_far[axis, k].append(
                    push(axis, s, block(ci, along[j], other[k], at), block(ci, along[3], other[k], at))
                )

    def down_near_forward(f, k):
        for axis, block, along, other in lines:
            for j in (1, 2):
                forward(fwd_d[f], lambda c: block(c, along[j], other[k]))

    def down_far_forward(f, k):
        for axis, block, along, other in lines:
            done(got_far[axis, k])
            forward(fwd_d[f], lambda c: block(c, along[3], other[k]))

    def near_wave(w):
        finish_near(second[w][0], fwd_gu[w], wave(a_gu, w), xi)
        finish_near(second[w][1], fwd_gu[w], wave(b_gu, w), zi)

    def far_wave(w):
        finish_far(second[w][0], fwd_gu[w], wave(a_gu, w), xi)
        finish_far(second[w][1], fwd_gu[w], wave(b_gu, w), zi)

    for ring in second[0]:
        ring.relay()
    for ring in second[1]:
        ring.relay()
    second.append(wave_rings(2))
    done(own_d)
    ad1 = Ring("z", lambda i, h: a_d.at[ci, xi, i, pl.ds(h * hr, hr)])
    bd1 = Ring("x", lambda i, h: b_d.at[ci, zi, i, pl.ds(h * hr, hr)])
    near_wave(0)
    toks.relay()
    far_wave(0)
    near_wave(1)
    toks.near()
    done(fwd_gu[0])

    def unit_rows(w, which, lo, hi):
        count = waves[w][1]
        pieces = []
        for seg in range(4):
            a, b = max(lo, seg * count), min(hi, (seg + 1) * count)
            if a < b:
                c, h = divmod(seg, 2)
                r = slice(waves[w][0] + a - seg * count, waves[w][0] + b - seg * count)
                ref = (a_gu, b_gu)[h]
                pieces.append(
                    cat(
                        [
                            ref[(c, x, z) + (which, r)] if h == 0 else ref[(c, z, x) + (which, r)]
                            for z, x in every
                        ],
                        1,
                    )
                )
        return cat(pieces, 0)

    step = 256
    places = [yi, wrap(yi, -1), wrap(yi, 1), wrap(yi, 2)]

    def hidden_tile(w, lo, first, last):
        count = 4 * waves[w][1]
        hi = min(lo + step, count)
        block = cat([xall[y] for y in places[first:last]], 0)
        if hi - lo == step:
            gate_pre = dot_nt(block, unit_rows(w, 0, lo, hi))
            up_pre = dot_nt(block, unit_rows(w, 1, lo, hi))
        else:
            weights = cat([unit_rows(w, 0, lo, hi), unit_rows(w, 1, lo, hi)], 0)
            middle_row = block.shape[0] // 2
            both = cat([dot_nt(b, weights) for b in (block[:middle_row], block[middle_row:])], 0)
            gate_pre, up_pre = both[:, : hi - lo], both[:, hi - lo :]
        at = 4 * waves[w][0]
        hidden[first * span : last * span, at + lo : at + hi] = (
            gate_pre * lax.logistic(gate_pre) * up_pre
        ).astype(BF)

    far_wave(1)
    hidden_tile(0, 0, 0, 3)
    hidden_tile(0, step, 0, 3)
    for ring in second[2]:
        ring.relay()
    down_send(0)
    done(fwd_gu[1])
    hidden_tile(1, 0, 0, 3)
    hidden_tile(1, step, 0, 3)
    near_wave(2)
    for ring in (ad1, bd1):
        ring.relay()
    toks.end()
    hidden_tile(0, 0, 3, 4)
    hidden_tile(0, step, 3, 4)
    for ring in (ad1, bd1):
        ring.near()
    down_send(1)
    down_send(2)
    for k in range(3):
        forward(fwd_d[0], lambda c: block_a(c, xi, places_z[k]))
        forward(fwd_d[0], lambda c: block_b(c, zi, places_x[k]))
    far_wave(2)
    hidden_tile(1, 0, 3, 4)
    hidden_tile(1, step, 3, 4)
    down_near(0)
    down_near_forward(1, 0)
    done(fwd_gu[2])
    hidden_tile(2, 0, 0, 4)
    hidden_tile(2, step, 0, 4)

    got_r1, got_r2 = {}, {}
    own, back, ahead, opposite = range(N)

    order = [(0, 0), (0, 1), (1, 0), (2, 0), (0, 2), (1, 1), (1, 2), (2, 1), (2, 2), (0, 3), (3, 0),
             (1, 3), (2, 3), (3, 1), (3, 2), (3, 3)]
    blocks = [(places_z[i], places_x[j]) for i, j in order]
    rounds = [(blocks[r], blocks[r + 1]) for r in range(0, len(blocks), 2)]

    def sum_first(r):
        low, high = rounds[r]
        got_r1[r] = [
            send_to("y", 1, parts.at[(opposite, *low)], r1.at[(0, *low)]),
            send_to("y", -1, parts.at[(opposite, *high)], r1.at[(1, *high)]),
        ]

    def sum_direct(r):
        low, high = rounds[r]
        got_r2[r] = [
            send_to("y", 1, parts.at[(ahead, *high)], r2.at[(0, *high)]),
            send_to("y", -1, parts.at[(back, *low)], r2.at[(1, *low)]),
        ]

    def send_to(axis, s, src, dst):
        k = len(sends)
        copy = pltpu.make_async_remote_copy(
            src, dst, ssem.at[k], rsem.at[k], device_id=device(axis, s),
            device_id_type=pl.DeviceIdType.MESH,
        )
        copy.start()
        sends.append(copy)
        return copy.wait_recv

    def sum_second(r):
        for k, (s, rel, at) in enumerate(((1, ahead, rounds[r][0]), (-1, back, rounds[r][1]))):
            got_r1[r][k]()
            parts[(rel, *at)] = (
                parts[(rel, *at)].astype(F32) + r1[(k, *at)].astype(F32)
            ).astype(BF)
            got_r2[r].append(send_to("y", s, parts.at[(rel, *at)], r2.at[(k, *at)]))

    def sum_last(r):
        done(got_r2[r])
        for z, x in rounds[r]:
            summed = (
                parts[own, z, x].astype(F32) + r2[0, z, x].astype(F32) + r2[1, z, x].astype(F32)
            )
            cols = pl.ds(pl.multiple_of((z * N + x) * lane, lane), lane)
            out[:, cols] = (middle[:, cols].astype(F32) + summed).astype(BF)

    def multiply(r):
        weights = cat(
            [
                cat(
                    [
                        ref
                        for off, count in waves
                        for c in range(2)
                        for ref in (a_d[c, x, z, off : off + count], b_d[c, z, x, off : off + count])
                    ],
                    0,
                )
                for z, x in rounds[r]
            ],
            1,
        )
        for y in range(0, N, 2):
            rows_y = hidden[y * span : (y + 2) * span, :]
            result = jnp.dot(rows_y, weights, preferred_element_type=F32).astype(BF)
            for i in range(2):
                for j, (z, x) in enumerate(rounds[r]):
                    parts[y + i, z, x] = result[
                        i * span : (i + 1) * span, j * lane : (j + 1) * lane
                    ]

    done(fwd_d[0])
    done(fwd_d[1])
    multiply(0)
    sum_first(0)
    multiply(1)
    sum_first(1)
    sum_direct(0)
    sum_direct(1)
    for ring in (ad1, bd1):
        ring.end()
    down_send(3)
    forward(fwd_d[4], lambda c: block_a(c, xi, places_z[3]))
    forward(fwd_d[4], lambda c: block_b(c, zi, places_x[3]))
    down_near(1)
    down_near_forward(2, 1)
    down_near(2)
    down_near_forward(3, 2)
    done(fwd_d[2])
    multiply(2)
    sum_first(2)
    sum_direct(2)
    down_far_forward(4, 0)
    done(fwd_d[3])
    multiply(3)
    sum_first(3)
    sum_second(0)
    sum_second(1)
    sum_direct(3)
    done(fwd_d[4])
    multiply(4)
    sum_first(4)
    down_near(3)
    down_near_forward(5, 3)
    sum_second(2)
    sum_direct(4)
    down_far_forward(6, 1)
    down_far_forward(6, 2)
    sum_second(3)
    done(fwd_d[5])
    done(fwd_d[6])
    multiply(5)
    sum_first(5)
    multiply(6)
    sum_first(6)
    sum_direct(5)
    down_far_forward(7, 3)
    sum_second(4)
    done(fwd_d[7])
    multiply(7)
    sum_first(7)
    sum_direct(6)
    sum_direct(7)
    sum_last(0)
    sum_last(1)
    sum_second(5)
    sum_second(6)
    sum_last(2)
    sum_last(3)
    early = len(sends) - 48
    for copy in sends[:early]:
        copy.wait_send()
    sum_second(7)
    sum_last(4)
    sum_last(5)
    sum_last(6)
    sum_last(7)
    assert len(sends) <= COPIES
    for copy in sends[early:]:
        copy.wait_send()


def per_device(
    tokens, mix_gain, gate_proj, value_proj, layer_gain, layer_shift, mix_kernel, mix_offset,
    out_proj, ffn_gain, ffn_gate, ffn_up, ffn_down,
):
    span, width = tokens.shape
    units, lane = ffn_gate.shape[1], ffn_gate.shape[0]
    local = gate_proj.shape[1]
    half = units // 2
    anywhere = pl.BlockSpec(memory_space=pl.ANY)
    return pl.pallas_call(
        kernel,
        out_shape=pltpu.VMEM(tokens.shape, BF),
        in_specs=[anywhere] * 13,
        out_specs=pl.BlockSpec(memory_space=pltpu.VMEM),
        scratch_shapes=[
            pltpu.VMEM((span, width), BF),
            pltpu.VMEM(mix_gain.shape, BF),
            pltpu.VMEM(ffn_gain.shape, BF),
            pltpu.VMEM(layer_gain.shape, BF),
            pltpu.VMEM(layer_shift.shape, BF),
            pltpu.VMEM(mix_offset.shape, BF),
            pltpu.VMEM(mix_kernel.shape, BF),
            pltpu.VMEM((2, N, N, N, local, lane), BF),
            pltpu.VMEM((2, N, N, N, local, lane), BF),
            pltpu.VMEM((2, N, N, N, local, lane), BF),
            pltpu.VMEM((2, N, N, 2, half, lane), BF),
            pltpu.VMEM((2, N, N, 2, half, lane), BF),
            pltpu.VMEM((2, N, N, half, lane), BF),
            pltpu.VMEM((2, N, N, half, lane), BF),
            pltpu.VMEM((span, width), BF),
            pltpu.VMEM((span, width), BF),
            pltpu.VMEM((N, span, width), BF),
            pltpu.VMEM((N * span, 2 * units), BF),
            pltpu.VMEM((N, N, N, span, lane), BF),
            pltpu.VMEM((2, N, N, span, lane), BF),
            pltpu.VMEM((2, N, N, span, lane), BF),
            pltpu.SemaphoreType.DMA((24,)),
            pltpu.SemaphoreType.DMA((COPIES,)),
            pltpu.SemaphoreType.DMA((COPIES,)),
        ],
        compiler_params=pltpu.CompilerParams(
            collective_id=0, has_side_effects=True, vmem_limit_bytes=63 * 2**20
        ),
    )(
        tokens, gate_proj.T, value_proj.T, out_proj.T, ffn_gate.T, ffn_up.T, ffn_down.T,
        mix_gain, layer_gain, layer_shift, mix_kernel, mix_offset, ffn_gain,
    )


def solution(mesh):
    torus = Mesh(mesh.devices.reshape(mesh.shape["rep"], 4, 4, 4, 2), AXES)
    return jax.shard_map(
        per_device,
        mesh=torus,
        in_specs=(
            P(AXES, None), P(), P(FS, TP), P(FS, TP), P(), P(), P(), P(), P(FS, TP), P(),
            P(FS, TP), P(FS, TP), P(FS, TP),
        ),
        out_specs=P(AXES, None),
        check_vma=False,
    )
```

```python
import functools

import jax
import jax.numpy as jnp
from jax import lax
from jax.experimental import pallas as pl
from jax.experimental.pallas import tpu as pltpu
from jax.sharding import Mesh
from jax.sharding import PartitionSpec as P

AXES = ("rep", "fs_0", "fs_1", "tp_0", "tp_1")
FS = ("fs_0", "fs_1")
TP = ("tp_0", "tp_1")
EPS = 1e-06
N = 4
COPIES = 280


def row_waves(half):
    return [(0, 128), (128, 128), (256, half - 256)]

BF, F32 = jnp.bfloat16, jnp.float32


def dot_nt(left, right):
    return lax.dot_general(left, right, (((1,), (1,)), ((), ())), preferred_element_type=F32)


def gelu(v):
    return v * (0.5 * (1.0 + jnp.tanh(0.7978845608028654 * (v + 0.044715 * (v * v * v)))))


def row(ref):
    return ref[...].astype(F32).reshape(1, -1)


def cat(parts, axis):
    return jnp.concatenate(parts, axis=axis) if len(parts) > 1 else parts[0]


def kernel(
    tokens, gate_proj, value_proj, out_proj, ffn_gate, ffn_up, ffn_down, mix_gain, layer_gain,
    layer_shift, mix_kernel, mix_offset, ffn_gain,
    out,
    tok, gain1, gain2, lgain, lshift, mixo, mixk, vw, gw, ow, a_gu, b_gu, a_d, b_d, nbuf, middle, xall, hidden, parts, r1, r2,
    lsem, ssem, rsem,
):
    rep = lax.axis_index("rep")
    zi, xi, yi, ci = (lax.axis_index(a) for a in AXES[1:])

    def wrap(i, s):
        return lax.rem(i + (s + N), N)

    def device(axis, s):
        if axis == "z":
            z = lax.rem(rep * N + zi + (s + 2 * N), 2 * N)
            return {"rep": z // N, "fs_0": lax.rem(z, N)}
        if axis == "c":
            return {"tp_1": 1 - ci}
        name, i = {"x": ("fs_1", xi), "y": ("tp_0", yi)}[axis]
        return {name: wrap(i, s)}

    index = {"x": xi, "y": yi, "z": zi}
    sends = []

    def push(axis, s, mine, theirs):
        k = len(sends)
        to = device(axis, s)
        copy = pltpu.make_async_remote_copy(
            mine, mine, ssem.at[k], rsem.at[k], device_id=to, device_id_type=pl.DeviceIdType.MESH
        )
        copy.start()
        sends.append(copy)
        arrival = pltpu.make_async_remote_copy(
            theirs, theirs, ssem.at[k], rsem.at[k], device_id=to,
            device_id_type=pl.DeviceIdType.MESH,
        )
        return arrival.wait_recv

    locals_ = []

    def load(src, dst):
        copy = pltpu.make_async_copy(src, dst, lsem.at[len(locals_)])
        copy.start()
        locals_.append(copy)
        return copy.wait

    half = a_d.shape[-2]
    hr = half // 2
    waves = row_waves(half)
    own_v = load(value_proj, vw.at[ci, yi, xi, zi])
    own_g = load(gate_proj, gw.at[ci, xi, zi, yi])
    own_o = load(out_proj, ow.at[ci, zi, yi, xi])
    own_gu = [
        load(src.at[pl.ds(h * half, half)], dst.at[j])
        for h, dst in ((0, a_gu.at[ci, xi, zi]), (1, b_gu.at[ci, zi, xi]))
        for j, src in ((0, ffn_gate), (1, ffn_up))
    ]
    got_tok = load(tokens, tok)
    own_d = [
        load(ffn_down.at[pl.ds(0, half)], a_d.at[ci, xi, zi]),
        load(ffn_down.at[pl.ds(half, half)], b_d.at[ci, zi, xi]),
    ]
    got_small = [
        load(src, dst)
        for src, dst in (
            (mix_gain, gain1), (layer_gain, lgain), (layer_shift, lshift), (mix_kernel, mixk),
            (mix_offset, mixo), (ffn_gain, gain2),
        )
    ]

    barrier = pltpu.get_barrier_semaphore()
    greeted = [(a, s) for a in "xyz" for s in (1, -1, 2)] + [("z", -2), ("c", 1)]
    for a, s in greeted:
        pl.semaphore_signal(
            barrier, inc=1, device_id=device(a, s), device_id_type=pl.DeviceIdType.MESH
        )
    pl.semaphore_wait(barrier, len(greeted))

    def direct(axis, group, halves):
        i = index[axis]
        got = [
            push(axis, 1, group(i), group(wrap(i, -1))),
            push(axis, -1, group(i), group(wrap(i, 1))),
        ]
        far = wrap(i, 2)
        if axis == "z":
            got += [push(axis, 2, halves(i, 0), halves(far, 0)),
                    push(axis, -2, halves(i, 1), halves(far, 1))]
        else:
            got += [push(axis, 2, group(i), group(far))]
        return got

    class Ring:
        def __init__(self, axis, halves):
            self.axis, self.halves, self.i = axis, halves, index[axis]
            i = self.i
            before, after = wrap(i, -1), wrap(i, 1)
            self.first = [push(axis, 1, halves(i, 0), halves(before, 0)),
                          push(axis, -1, halves(i, 1), halves(after, 1))]
            self.second = [push(axis, 1, halves(i, 1), halves(before, 1)),
                           push(axis, -1, halves(i, 0), halves(after, 0))]

        def relay(self):
            i, h = self.i, self.halves
            before, after, far = wrap(i, -1), wrap(i, 1), wrap(i, 2)
            self.first[0]()
            up = push(self.axis, 1, h(before, 0), h(far, 0))
            self.first[1]()
            down = push(self.axis, -1, h(after, 1), h(far, 1))
            self.last = [up, down]

        def near(self):
            for w in self.second:
                w()

        def end(self):
            for w in self.last:
                w()

    def pair(n):
        return lambda h: pl.ds(h * (n // 2), n // 2)

    rows = pair(vw.shape[-2])
    two = pair(N)
    own_v()
    v1 = direct("z", lambda i: vw.at[ci, yi, xi, i], lambda i, h: vw.at[ci, yi, xi, i, rows(h)])
    own_g()
    g1 = direct("y", lambda i: gw.at[ci, xi, zi, i], None)
    own_o()
    o1 = direct("x", lambda i: ow.at[ci, zi, yi, i], None)

    def wave(ref, w):
        off, count = waves[w]
        return lambda c, i: ref.at[c, i, :, :, pl.ds(off, count)]

    def wave_rings(w):
        off, count = waves[w]
        for ref, i in ((a_gu, xi), (b_gu, zi)):
            forward(fwd_gu[w], lambda c: wave(ref, w)(c, i))
        return (
            Ring("x", lambda i, h: a_gu.at[ci, i, two(h), :, pl.ds(off, count)]),
            Ring("z", lambda i, h: b_gu.at[ci, i, two(h), :, pl.ds(off, count)]),
        )

    def done(waits):
        for w in waits:
            w()

    def forward(keep, ref_of):
        keep.append(push("c", 1, ref_of(ci), ref_of(1 - ci)))

    def group(ref):
        return lambda c, i: ref.at[c, i]

    def finish_near(ring, keep, of, i):
        ring.near()
        forward(keep, lambda c: of(c, wrap(i, -1)))
        forward(keep, lambda c: of(c, wrap(i, 1)))

    def finish_far(ring, keep, of, i):
        ring.end()
        forward(keep, lambda c: of(c, wrap(i, 2)))

    fwd_v, fwd_g, fwd_o, fwd_gu = [], [], [], [[], [], []]
    done(own_gu)
    first = (Ring("z", lambda i, h: a_gu.at[ci, xi, i, h]),
             Ring("x", lambda i, h: b_gu.at[ci, zi, i, h]))
    done(v1)
    v2 = direct("x", lambda i: vw.at[ci, yi, i], None)
    done(g1)
    g2 = direct("z", lambda i: gw.at[ci, xi, i], lambda i, h: gw.at[ci, xi, i, two(h)])
    done(o1)
    o2 = direct("y", lambda i: ow.at[ci, zi, i], None)
    for ring in first:
        ring.relay()
    done(v2)
    v3 = Ring("y", lambda i, h: vw.at[ci, i, two(h)])
    forward(fwd_v, lambda c: vw.at[c, yi])
    done(g2)
    g3 = Ring("x", lambda i, h: gw.at[ci, i, two(h)])
    forward(fwd_g, lambda c: gw.at[c, xi])
    done(o2)
    o3 = Ring("z", lambda i, h: ow.at[ci, i, two(h)])
    forward(fwd_o, lambda c: ow.at[c, zi])

    got_tok()
    done(got_small)
    floats = tok[...].astype(F32)
    scale = lax.rsqrt(jnp.mean(floats * floats, axis=-1, keepdims=True) + EPS)
    nbuf[...] = (floats * scale * row(gain1)).astype(BF)

    v3.relay()
    g3.relay()
    o3.relay()
    for ring in first:
        ring.near()
        ring.end()
    second = [wave_rings(0), wave_rings(1)]
    finish_near(v3, fwd_v, group(vw), yi)
    finish_far(v3, fwd_v, group(vw), yi)
    finish_near(g3, fwd_g, group(gw), xi)
    finish_near(o3, fwd_o, group(ow), zi)
    done(fwd_v)

    every = [(z, x) for z in range(N) for x in range(N)]

    def project(block, lo):
        cols = [
            cat([block(c, y, z, x) for y in (lo, lo + 1) for c in range(2)], 0) for z, x in every
        ]
        return dot_nt(nbuf[...], cat(cols, 1))

    width = 512
    activated = gelu(cat([project(lambda c, y, z, x: vw[c, y, x, z], lo) for lo in (0, 2)], 1))
    center = jnp.sum(activated, axis=-1, keepdims=True) / width
    spread = jnp.sum(activated * activated, axis=-1, keepdims=True) / width - center * center
    values = (
        (activated - center) * lax.rsqrt(spread + EPS) * row(lgain) + row(lshift)
    ).astype(BF)
    done(fwd_g[:3])
    ring_x = [xi, wrap(xi, -1), wrap(xi, 1), wrap(xi, 2)]

    def gate_part(xs):
        pairs = [(z, x) for z in range(N) for x in xs]
        left = cat(
            [nbuf[:, pl.ds(pl.multiple_of((z * N + x) * 128, 128), 128)] for z, x in pairs], 1
        )
        return cat(
            [
                dot_nt(
                    left,
                    cat(
                        [
                            cat([gw[c, x, z, y] for y in (lo, lo + 1) for c in range(2)], 0)
                            for z, x in pairs
                        ],
                        1,
                    ),
                )
                for lo in (0, 2)
            ],
            1,
        )

    gate_near = gate_part(ring_x[:3])
    finish_far(g3, fwd_g, group(gw), xi)
    finish_far(o3, fwd_o, group(ow), zi)
    span, groups = mixk.shape[1], mixk.shape[0]
    t_pos = lax.broadcasted_iota(jnp.int32, (span, span), 0)
    s_pos = lax.broadcasted_iota(jnp.int32, (span, span), 1)
    mixing = []
    for g in range(groups):
        masked = jnp.where(s_pos <= t_pos, mixk[g].astype(F32), 0.0).astype(BF)
        offset_row = mixo[g : g + 1, :].astype(F32)
        offset = jnp.sum(jnp.where(s_pos == t_pos, offset_row, 0.0), axis=-1, keepdims=True)
        mixing.append(
            jnp.dot(masked, values[:, g * span : (g + 1) * span], preferred_element_type=F32)
            + offset
        )
    done(fwd_g[3:])
    gate_u = gelu(gate_near + gate_part(ring_x[3:]))
    gated = (gate_u * cat(mixing, 1)).astype(BF)
    done(fwd_o)
    total = jnp.zeros((span, 1), F32)
    lane = 128
    for z in range(N):
        weights = cat(
            [
                cat([ow[c, z, y, x] for y in range(N) for c in range(2)], 0)
                for x in range(N)
            ],
            1,
        )
        cols = slice(z * N * lane, (z + 1) * N * lane)
        mid = (
            tok[:, cols].astype(F32) + jnp.dot(gated, weights, preferred_element_type=F32)
        ).astype(BF)
        middle[:, cols] = mid
        mid = mid.astype(F32)
        total += jnp.sum(mid * mid, axis=-1, keepdims=True)
    width2 = middle.shape[1]
    scale2 = lax.rsqrt(total / width2 + EPS)
    xall[yi] = (middle[...].astype(F32) * scale2 * row(gain2)).astype(BF)

    toks = Ring("y", lambda i, h: xall.at[i, pl.ds(h * (span // 2), span // 2)])

    places_x = [xi, wrap(xi, -1), wrap(xi, 1), wrap(xi, 2)]
    places_z = [zi, wrap(zi, -1), wrap(zi, 1), wrap(zi, 2)]
    got_near, got_far = {}, {}
    fwd_d = [[] for _ in range(8)]

    def block_a(c, x, z, at=pl.ds(0, half)):
        return a_d.at[c, x, z, at]

    def block_b(c, z, x, at=pl.ds(0, half)):
        return b_d.at[c, z, x, at]

    lines = (("x", block_a, places_x, places_z), ("z", block_b, places_z, places_x))

    def down_send(k):
        for axis, block, along, other in lines:
            mine = block(ci, along[0], other[k])
            got_near[axis, k] = [push(axis, 1, mine, block(ci, along[1], other[k])),
                                 push(axis, -1, mine, block(ci, along[2], other[k]))]

    def down_near(k):
        for axis, block, along, other in lines:
            got_far[axis, k] = []
            for h, (w, s, j) in enumerate(zip(got_near[axis, k], (1, -1), (1, 2))):
                w()
                at = pl.ds(h * hr, hr)
                got_far[axis, k].append(
                    push(axis, s, block(ci, along[j], other[k], at), block(ci, along[3], other[k], at))
                )

    def down_near_forward(f, k):
        for axis, block, along, other in lines:
            for j in (1, 2):
                forward(fwd_d[f], lambda c: block(c, along[j], other[k]))

    def down_far_forward(f, k):
        for axis, block, along, other in lines:
            done(got_far[axis, k])
            forward(fwd_d[f], lambda c: block(c, along[3], other[k]))

    def near_wave(w):
        finish_near(second[w][0], fwd_gu[w], wave(a_gu, w), xi)
        finish_near(second[w][1], fwd_gu[w], wave(b_gu, w), zi)

    def far_wave(w):
        finish_far(second[w][0], fwd_gu[w], wave(a_gu, w), xi)
        finish_far(second[w][1], fwd_gu[w], wave(b_gu, w), zi)

    for ring in second[0]:
        ring.relay()
    for ring in second[1]:
        ring.relay()
    second.append(wave_rings(2))
    done(own_d)
    ad1 = Ring("z", lambda i, h: a_d.at[ci, xi, i, pl.ds(h * hr, hr)])
    bd1 = Ring("x", lambda i, h: b_d.at[ci, zi, i, pl.ds(h * hr, hr)])
    near_wave(0)
    toks.relay()
    far_wave(0)
    near_wave(1)
    toks.near()
    done(fwd_gu[0])

    def unit_rows(w, which, lo, hi):
        count = waves[w][1]
        pieces = []
        for seg in range(4):
            a, b = max(lo, seg * count), min(hi, (seg + 1) * count)
            if a < b:
                c, h = divmod(seg, 2)
                r = slice(waves[w][0] + a - seg * count, waves[w][0] + b - seg * count)
                ref = (a_gu, b_gu)[h]
                pieces.append(
                    cat(
                        [
                            ref[(c, x, z) + (which, r)] if h == 0 else ref[(c, z, x) + (which, r)]
                            for z, x in every
                        ],
                        1,
                    )
                )
        return cat(pieces, 0)

    step = 256
    places = [yi, wrap(yi, -1), wrap(yi, 1), wrap(yi, 2)]

    def hidden_tile(w, lo, first, last):
        count = 4 * waves[w][1]
        hi = min(lo + step, count)
        block = cat([xall[y] for y in places[first:last]], 0)
        if hi - lo == step:
            gate_pre = dot_nt(block, unit_rows(w, 0, lo, hi))
            up_pre = dot_nt(block, unit_rows(w, 1, lo, hi))
        else:
            weights = cat([unit_rows(w, 0, lo, hi), unit_rows(w, 1, lo, hi)], 0)
            middle_row = block.shape[0] // 2
            both = cat([dot_nt(b, weights) for b in (block[:middle_row], block[middle_row:])], 0)
            gate_pre, up_pre = both[:, : hi - lo], both[:, hi - lo :]
        at = 4 * waves[w][0]
        hidden[first * span : last * span, at + lo : at + hi] = (
            gate_pre * lax.logistic(gate_pre) * up_pre
        ).astype(BF)

    far_wave(1)
    hidden_tile(0, 0, 0, 3)
    hidden_tile(0, step, 0, 3)
    for ring in second[2]:
        ring.relay()
    down_send(0)
    done(fwd_gu[1])
    hidden_tile(1, 0, 0, 3)
    hidden_tile(1, step, 0, 3)
    near_wave(2)
    for ring in (ad1, bd1):
        ring.relay()
    toks.end()
    hidden_tile(0, 0, 3, 4)
    hidden_tile(0, step, 3, 4)
    for ring in (ad1, bd1):
        ring.near()
    down_send(1)
    down_send(2)
    for k in range(3):
        forward(fwd_d[0], lambda c: block_a(c, xi, places_z[k]))
        forward(fwd_d[0], lambda c: block_b(c, zi, places_x[k]))
    far_wave(2)
    hidden_tile(1, 0, 3, 4)
    hidden_tile(1, step, 3, 4)
    down_near(0)
    down_near_forward(1, 0)
    done(fwd_gu[2])
    hidden_tile(2, 0, 1, 4)
    hidden_tile(2, step, 1, 4)

    got_r1, got_r2 = {}, {}
    own, back, ahead, opposite = range(N)

    order = [(0, 0), (0, 1), (1, 0), (2, 0), (0, 2), (1, 1), (1, 2), (2, 1), (2, 2), (0, 3), (3, 0),
             (1, 3), (2, 3), (3, 1), (3, 2), (3, 3)]
    blocks = [(places_z[i], places_x[j]) for i, j in order]
    rounds = [(blocks[r], blocks[r + 1]) for r in range(0, len(blocks), 2)]

    def sum_first(r):
        low, high = rounds[r]
        got_r1[r] = [
            send_to("y", 1, parts.at[(opposite, *low)], r1.at[(0, *low)]),
            send_to("y", -1, parts.at[(opposite, *high)], r1.at[(1, *high)]),
        ]

    def sum_direct(r):
        low, high = rounds[r]
        got_r2[r] = [
            send_to("y", 1, parts.at[(ahead, *high)], r2.at[(0, *high)]),
            send_to("y", -1, parts.at[(back, *low)], r2.at[(1, *low)]),
        ]

    def send_to(axis, s, src, dst):
        k = len(sends)
        copy = pltpu.make_async_remote_copy(
            src, dst, ssem.at[k], rsem.at[k], device_id=device(axis, s),
            device_id_type=pl.DeviceIdType.MESH,
        )
        copy.start()
        sends.append(copy)
        return copy.wait_recv

    def sum_second(r):
        for k, (s, rel, at) in enumerate(((1, ahead, rounds[r][0]), (-1, back, rounds[r][1]))):
            got_r1[r][k]()
            parts[(rel, *at)] = (
                parts[(rel, *at)].astype(F32) + r1[(k, *at)].astype(F32)
            ).astype(BF)
            got_r2[r].append(send_to("y", s, parts.at[(rel, *at)], r2.at[(k, *at)]))

    def sum_last(r):
        done(got_r2[r])
        for z, x in rounds[r]:
            summed = (
                parts[own, z, x].astype(F32) + r2[0, z, x].astype(F32) + r2[1, z, x].astype(F32)
            )
            cols = pl.ds(pl.multiple_of((z * N + x) * lane, lane), lane)
            out[:, cols] = (middle[:, cols].astype(F32) + summed).astype(BF)

    def multiply(r, pieces=((0, 2), (2, 4))):
        weights = cat(
            [
                cat(
                    [
                        ref
                        for off, count in waves
                        for c in range(2)
                        for ref in (a_d[c, x, z, off : off + count], b_d[c, z, x, off : off + count])
                    ],
                    0,
                )
                for z, x in rounds[r]
            ],
            1,
        )
        for y, end in pieces:
            rows_y = hidden[y * span : end * span, :]
            result = jnp.dot(rows_y, weights, preferred_element_type=F32).astype(BF)
            for i in range(end - y):
                for j, (z, x) in enumerate(rounds[r]):
                    parts[y + i, z, x] = result[
                        i * span : (i + 1) * span, j * lane : (j + 1) * lane
                    ]

    done(fwd_d[0])
    done(fwd_d[1])
    sent = ((1, 2), (2, 4))
    multiply(0, sent)
    sum_first(0)
    multiply(1, sent)
    sum_first(1)
    sum_direct(0)
    sum_direct(1)
    for ring in (ad1, bd1):
        ring.end()
    down_send(3)
    forward(fwd_d[4], lambda c: block_a(c, xi, places_z[3]))
    forward(fwd_d[4], lambda c: block_b(c, zi, places_x[3]))
    down_near(1)
    down_near_forward(2, 1)
    down_near(2)
    down_near_forward(3, 2)
    hidden_tile(2, 0, 0, 1)
    hidden_tile(2, step, 0, 1)
    done(fwd_d[2])
    multiply(2)
    sum_first(2)
    sum_direct(2)
    down_far_forward(4, 0)
    done(fwd_d[3])
    multiply(3)
    sum_first(3)
    sum_second(0)
    sum_second(1)
    sum_direct(3)
    done(fwd_d[4])
    multiply(4)
    sum_first(4)
    down_near(3)
    down_near_forward(5, 3)
    sum_second(2)
    sum_direct(4)
    down_far_forward(6, 1)
    down_far_forward(6, 2)
    sum_second(3)
    done(fwd_d[5])
    done(fwd_d[6])
    multiply(5)
    sum_first(5)
    multiply(6)
    sum_first(6)
    sum_direct(5)
    down_far_forward(7, 3)
    sum_second(4)
    done(fwd_d[7])
    multiply(7)
    sum_first(7)
    sum_direct(6)
    sum_direct(7)
    multiply(0, ((0, 1),))
    multiply(1, ((0, 1),))
    sum_last(0)
    sum_last(1)
    sum_second(5)
    sum_second(6)
    sum_last(2)
    sum_last(3)
    early = len(sends) - 48
    for copy in sends[:early]:
        copy.wait_send()
    sum_second(7)
    sum_last(4)
    sum_last(5)
    sum_last(6)
    sum_last(7)
    assert len(sends) <= COPIES
    for copy in sends[early:]:
        copy.wait_send()


def per_device(
    tokens, mix_gain, gate_proj, value_proj, layer_gain, layer_shift, mix_kernel, mix_offset,
    out_proj, ffn_gain, ffn_gate, ffn_up, ffn_down,
):
    span, width = tokens.shape
    units, lane = ffn_gate.shape[1], ffn_gate.shape[0]
    local = gate_proj.shape[1]
    half = units // 2
    anywhere = pl.BlockSpec(memory_space=pl.ANY)
    return pl.pallas_call(
        kernel,
        out_shape=pltpu.VMEM(tokens.shape, BF),
        in_specs=[anywhere] * 13,
        out_specs=pl.BlockSpec(memory_space=pltpu.VMEM),
        scratch_shapes=[
            pltpu.VMEM((span, width), BF),
            pltpu.VMEM(mix_gain.shape, BF),
            pltpu.VMEM(ffn_gain.shape, BF),
            pltpu.VMEM(layer_gain.shape, BF),
            pltpu.VMEM(layer_shift.shape, BF),
            pltpu.VMEM(mix_offset.shape, BF),
            pltpu.VMEM(mix_kernel.shape, BF),
            pltpu.VMEM((2, N, N, N, local, lane), BF),
            pltpu.VMEM((2, N, N, N, local, lane), BF),
            pltpu.VMEM((2, N, N, N, local, lane), BF),
            pltpu.VMEM((2, N, N, 2, half, lane), BF),
            pltpu.VMEM((2, N, N, 2, half, lane), BF),
            pltpu.VMEM((2, N, N, half, lane), BF),
            pltpu.VMEM((2, N, N, half, lane), BF),
            pltpu.VMEM((span, width), BF),
            pltpu.VMEM((span, width), BF),
            pltpu.VMEM((N, span, width), BF),
            pltpu.VMEM((N * span, 2 * units), BF),
            pltpu.VMEM((N, N, N, span, lane), BF),
            pltpu.VMEM((2, N, N, span, lane), BF),
            pltpu.VMEM((2, N, N, span, lane), BF),
            pltpu.SemaphoreType.DMA((24,)),
            pltpu.SemaphoreType.DMA((COPIES,)),
            pltpu.SemaphoreType.DMA((COPIES,)),
        ],
        compiler_params=pltpu.CompilerParams(
            collective_id=0, has_side_effects=True, vmem_limit_bytes=63 * 2**20
        ),
    )(
        tokens, gate_proj.T, value_proj.T, out_proj.T, ffn_gate.T, ffn_up.T, ffn_down.T,
        mix_gain, layer_gain, layer_shift, mix_kernel, mix_offset, ffn_gain,
    )


def solution(mesh):
    torus = Mesh(mesh.devices.reshape(mesh.shape["rep"], 4, 4, 4, 2), AXES)
    return jax.shard_map(
        per_device,
        mesh=torus,
        in_specs=(
            P(AXES, None), P(), P(FS, TP), P(FS, TP), P(), P(), P(), P(), P(FS, TP), P(),
            P(FS, TP), P(FS, TP), P(FS, TP),
        ),
        out_specs=P(AXES, None),
        check_vma=False,
    )
```
